128 devices in a mesh: kv: 16 (over z, x), tp: 8 (over y, core).
Axes of the slice: x: 4, y: 4, z: 4, core: 2. Of those that a mesh axis runs over, the one named last changes fastest.
Arguments:
- hidden: bfloat16 [1024, 4096], P(None, 'kv'), as said below
- norm_gain: bfloat16 [4096], replicated, may hold values from 0.099609375 to 1.8984375
- w_query: bfloat16 [4096, 4096], P('kv', 'tp'), may hold values from -0.09375 to 0.09375
- w_key: bfloat16 [4096, 4096], P('kv', 'tp'), may hold values from -0.09375 to 0.09375
- w_value: bfloat16 [4096, 8192], P('kv', 'tp'), may hold values from -0.09375 to 0.09375
- w_gate: bfloat16 [4096, 8192], P('kv', 'tp'), may hold values from -0.09375 to 0.09375
- w_write: bfloat16 [4096, 32], P('kv', 'tp'), may hold values from -0.09375 to 0.09375
- w_decay: bfloat16 [4096, 32], P('kv', 'tp'), may hold values from -0.09375 to 0.09375
- w_out: bfloat16 [8192, 4096], P('tp', 'kv'), may hold values from -0.0625 to 0.0625
- decay_rate: float32 [32], P('tp'), may hold values from 0 to 4, as said below
- head_gain: float32 [256], replicated, may hold values from 0.1 to 1.9
- carried_state: float32 [256, 32, 128, 256], P('kv', 'tp'), may hold values from -4 to 4
- last_keys: bfloat16 [256, 4, 4096], P('kv', None, 'tp'), may hold values from -6 to 6
- last_values: bfloat16 [256, 4, 8192], P('kv', None, 'tp'), may hold values from -6 to 6
- last_writes: float32 [256, 4, 32], P('kv', None, 'tp'), may hold values from -6 to 6
- last_decays: float32 [256, 4, 32], P('kv', None, 'tp'), may hold values from -6 to 6
- accepted: int32 [256], P('kv'), may hold values from 0 to 4
Outputs:
- mixed_out: bfloat16 [1024, 4096], P('tp', 'kv')
- committed: float32 [256, 32, 128, 256], P('kv', 'tp')
The draws below stay inside these ranges and needn't reach their ends.
Inputs may be any that keep to these rules, and one draw needn't show every extreme that they name: `decay_rate`: positive. `hidden`: finite real values.
All inputs are finite; a program needn't handle non-finite values.
Results may differ from the reference program's by a relative error of at most 0.029.
Values may be sent and summed in bfloat16 or wider, within the bound.
A program may use at most 128 MiB of HBM per device.

```python
import math
import jax
import jax.numpy as jnp
from jax import lax

D = 4096
HEADS = 32
DK = 128
DV = 256
PROP = 4
SEQS = 256
TOKENS = 1024
N_TP = 8


def draw_hidden(key, part):
    first, second, third = jax.random.split(key, 3)
    group = max(D // 16, 1)
    groups = (D + group - 1) // group
    scales = jnp.exp(jax.random.uniform(first, (groups,), jnp.float32, math.log(0.25), math.log(4.0)))
    channel_scale = scales[jnp.arange(D) // group]
    base = jax.random.normal(second, (TOKENS, D), jnp.float32)
    return (base * channel_scale[None, :]).astype(jnp.bfloat16)


def draw_decay_rate(key, part):
    return jnp.exp(jax.random.uniform(key, (HEADS,), jnp.float32, math.log(0.02), math.log(4.0)))


def with_ends(entries, own_key, smallest, largest):
    dims = entries.shape
    spot = [jax.random.randint(jax.random.fold_in(own_key, axis), (), 0, dims[axis]) for axis in range(len(dims))]
    entries = entries.at[tuple(spot)].set(smallest)
    longest = dims.index(max(dims))
    spot[longest] = (spot[longest] + 1) % dims[longest]
    return entries.at[tuple(spot)].set(largest)


def steps_of(rng, extent, cuts, low, top_value):
    loudness = 1.0
    for axis_at, shards_of in cuts:
        draws = jax.random.uniform(jax.random.fold_in(jax.random.fold_in(rng, 6), axis_at), (shards_of,), jnp.float32, low / len(cuts), top_value / len(cuts))
        loudness = loudness * jnp.repeat(jnp.exp(draws), extent[axis_at] // shards_of).reshape((-1,) + (1,) * (len(extent) - 1 - axis_at))
    return loudness


def gaussian(stream_key, dims, deviation, most, cuts=(), held_as=jnp.bfloat16):
    array = jax.random.normal(stream_key, dims, jnp.float32) * deviation
    if len(cuts) > 0:
        array = steps_of(stream_key, dims, cuts, -0.22, 0.18) * array
    return jnp.clip(array, min=-most, max=most).astype(held_as)


def setup_inputs(seed: int = 0) -> dict:
    streams_of = jax.random.split(jax.random.key(seed), 18)
    return {
        "hidden": draw_hidden(jax.random.fold_in(streams_of[17], 71), 0),
        "norm_gain": jnp.clip(1.0 + 0.18 * jax.random.normal(streams_of[1], (D,), jnp.float32), 0.099609375, 1.8984375).astype(jnp.bfloat16),
        "w_query": gaussian(streams_of[2], (D, HEADS * DK), D ** -0.5, 0.09375, ((0, 16), (1, 8))),
        "w_key": gaussian(streams_of[3], (D, HEADS * DK), D ** -0.5, 0.09375, ((0, 16), (1, 8))),
        "w_value": gaussian(streams_of[4], (D, HEADS * DV), D ** -0.5, 0.09375, ((0, 16), (1, 8))),
        "w_gate": gaussian(streams_of[5], (D, HEADS * DV), D ** -0.5, 0.09375, ((0, 16), (1, 8))),
        "w_write": gaussian(streams_of[6], (D, HEADS), D ** -0.5, 0.09375, ((0, 16), (1, 8))),
        "w_decay": gaussian(streams_of[7], (D, HEADS), D ** -0.5, 0.09375, ((0, 16), (1, 8))),
        "w_out": gaussian(streams_of[8], (HEADS * DV, D), (HEADS * DV) ** -0.5, 0.0625, ((0, 8), (1, 16))),
        "decay_rate": draw_decay_rate(jax.random.fold_in(streams_of[17], 71), 0),
        "head_gain": jnp.clip(1.0 + 0.18 * jax.random.normal(streams_of[10], (DV,), jnp.float32), 0.1, 1.9),
        "carried_state": gaussian(streams_of[11], (SEQS, HEADS, DK, DV), 0.3, 4.0, ((0, 16), (1, 8)), jnp.float32),
        "last_keys": gaussian(streams_of[12], (SEQS, PROP, HEADS * DK), 1.0, 6.0, ((0, 16), (2, 8))),
        "last_values": gaussian(streams_of[13], (SEQS, PROP, HEADS * DV), 1.0, 6.0, ((0, 16), (2, 8))),
        "last_writes": gaussian(streams_of[14], (SEQS, PROP, HEADS), 1.0, 6.0, ((0, 16), (2, 8)), jnp.float32),
        "last_decays": gaussian(streams_of[15], (SEQS, PROP, HEADS), 1.0, 6.0, ((0, 16), (2, 8)), jnp.float32),
        "accepted": with_ends(jax.random.randint(streams_of[16], (SEQS,), 0, PROP + 1), jax.random.fold_in(streams_of[16], 1), 0, PROP).astype(jnp.int32),
    }


norm_eps = 1e-06
highest = lax.Precision.HIGHEST

def unit_rows(matrix):
    return matrix * lax.rsqrt(lax.optimization_barrier(jnp.sum(matrix * matrix, -1, keepdims=True)) + norm_eps)

def corrected(key_rows, values, write_rate, log_decay, start_state):
    proposals = key_rows.shape[2]
    value_width = values.shape[-1]
    running = jnp.cumsum(log_decay, axis=-1)
    causal = jnp.tril(jnp.ones((proposals, proposals), dtype=bool))
    spread = running[..., :, None] - running[..., None, :]
    weights = jnp.where(causal, jnp.exp(jnp.where(causal, spread, 0.0)), 0.0)
    strong_keys = key_rows * write_rate[..., None]
    lower_part = jnp.einsum('bhcd,bhsd->bhcs', strong_keys, key_rows, precision=highest)
    lower_part = lower_part * weights * (1.0 - jnp.eye(proposals, dtype=jnp.float32))
    right_side = jnp.concatenate([values * write_rate[..., None], strong_keys * jnp.exp(running)[..., None]], -1)
    solved_rows = []
    for later in range(proposals):
        current = right_side[..., later, :]
        for early in range(later):
            current = current - lower_part[..., later, early, None] * solved_rows[early]
        solved_rows.append(current)
    solved = jnp.stack(solved_rows, axis=2)
    fresh_values = solved[..., :value_width] - jnp.einsum('bhcd,bhde->bhce', solved[..., value_width:], start_state, precision=highest)
    return (fresh_values, running, weights)

def advance(key_rows, fresh_values, running, start_state):
    tail_decay = jnp.exp(running[..., -1:] - running)
    return start_state * jnp.exp(running[..., -1])[..., None, None] + jnp.einsum('bhcd,bhce->bhde', key_rows * tail_decay[..., None], fresh_values, precision=highest)

def readout(queries, key_rows, fresh_values, running, weights, start_state):
    scores = jnp.einsum('bhcd,bhsd->bhcs', queries, key_rows, precision=highest) * weights
    carried = jnp.einsum('bhcd,bhde->bhce', queries * jnp.exp(running)[..., None], start_state, precision=highest)
    return carried + jnp.einsum('bhcs,bhse->bhce', scores, fresh_values, precision=highest)

def core(proj_query, proj_key, proj_value, proj_gate, proj_write, proj_decay, decay_rate, head_gain, carried_state, last_keys, last_values, last_writes, last_decays, accepted):
    seq_count, head_count, key_width, value_width = carried_state.shape
    proposals = last_keys.shape[1]

    def by_head(matrix, width):
        return jnp.transpose(matrix.reshape(seq_count, proposals, head_count, width), (0, 2, 1, 3))

    def by_head_small(matrix):
        return jnp.transpose(matrix.reshape(seq_count, proposals, head_count), (0, 2, 1))
    rates = decay_rate.astype(jnp.float32)[None, :, None]
    taken = (jnp.arange(proposals, dtype=jnp.int32)[None, :] < accepted[:, None]).astype(jnp.float32)[:, None, :]
    old_keys = unit_rows(by_head(last_keys.astype(jnp.float32), key_width))
    old_values = by_head(last_values.astype(jnp.float32), value_width)
    old_write = jax.nn.sigmoid(by_head_small(last_writes)) * taken
    old_decay = -rates * jax.nn.softplus(by_head_small(last_decays)) * taken
    fresh_values, running, weights = corrected(old_keys, old_values, old_write, old_decay, carried_state)
    committed = advance(old_keys, fresh_values, running, carried_state)
    queries = unit_rows(by_head(jax.nn.silu(proj_query), key_width)) * key_width ** (-0.5)
    key_rows = unit_rows(by_head(jax.nn.silu(proj_key), key_width))
    values = by_head(jax.nn.silu(proj_value), value_width)
    write_rate = jax.nn.sigmoid(by_head_small(proj_write))
    log_decay = -rates * jax.nn.softplus(by_head_small(proj_decay))
    fresh_values, running, weights = corrected(key_rows, values, write_rate, log_decay, committed)
    result = readout(queries, key_rows, fresh_values, running, weights, committed)
    normed = result * lax.rsqrt(lax.optimization_barrier(jnp.mean(result * result, -1, keepdims=True)) + norm_eps) * head_gain.astype(jnp.float32)
    gated = normed * jax.nn.silu(by_head(proj_gate, value_width))
    gated_rows = jnp.transpose(gated, (0, 2, 1, 3)).reshape(seq_count * proposals, head_count * value_width).astype(jnp.bfloat16)
    return (gated_rows, committed)

def reference(hidden, norm_gain, w_query, w_key, w_value, w_gate, w_write, w_decay, w_out, decay_rate, head_gain, carried_state, last_keys, last_values, last_writes, last_decays, accepted):
    wide_rows = hidden.astype(jnp.float32)
    inverse = lax.rsqrt(lax.optimization_barrier(jnp.sum(wide_rows * wide_rows, -1, keepdims=True)) / D + norm_eps)
    scaled = (wide_rows * norm_gain.astype(jnp.float32)).astype(jnp.bfloat16)

    def project(weight):
        return jnp.dot(scaled, weight, preferred_element_type=jnp.float32) * inverse
    gated_rows, committed = core(project(w_query), project(w_key), project(w_value), project(w_gate), project(w_write), project(w_decay), decay_rate, head_gain, carried_state, last_keys, last_values, last_writes, last_decays, accepted)
    grouped = gated_rows.astype(jnp.float32).reshape(TOKENS, N_TP, -1)
    weight_groups = w_out.astype(jnp.float32).reshape(N_TP, -1, D)
    partial_value = jnp.einsum('tmc,mcd->mtd', grouped, weight_groups)
    rounded = lax.optimization_barrier(partial_value.astype(jnp.bfloat16)).astype(jnp.float32)
    mixed_out = lax.optimization_barrier(jnp.sum(rounded, 0)).astype(jnp.bfloat16)
    return (mixed_out, committed)
```

```python
import functools

import jax
import jax.numpy as jnp
from jax import lax
from jax.experimental import pallas as pl
from jax.experimental.pallas import tpu as pltpu
from jax.sharding import PartitionSpec as P

MESH = pl.DeviceIdType.MESH
HIGHEST = lax.Precision.HIGHEST
F32 = jnp.float32
BF16 = jnp.bfloat16
norm_eps = 1e-06

TOK = 1024
OWN = 64
SEQ = 16
HD = 4
DK = 128
DV = 256
KB = 256
D = 4096
COLS = 2 * DK + 2 * DV


def softplus(x):
    return jnp.maximum(x, 0.0) + jnp.log1p(jnp.exp(-jnp.abs(x)))


def sigmoid(x):
    return 1.0 / (1.0 + jnp.exp(-x))


def silu(x):
    return x * sigmoid(x)


def place(shape):
    return lax.rem(lax.broadcasted_iota(jnp.int32, shape, 0), 4)


def back(x, j):
    return x if j == 0 else pltpu.roll(x, j, 0)


def ahead(x, j):
    return pltpu.roll(x, x.shape[0] - j, 0)


def wide(col, width):
    return jnp.broadcast_to(col, (col.shape[0], width))


def running_sum(g, at):
    c = g
    for j in (1, 2, 3):
        c = c + jnp.where(at >= j, back(g, j), 0.0)
    return c


def tail_sum(g, at):
    s = jnp.zeros_like(g)
    for j in (1, 2, 3):
        s = s + jnp.where(at + j <= 3, ahead(g, j), 0.0)
    return s


def unit(x):
    return x * lax.rsqrt(jnp.sum(x * x, -1, keepdims=True) + norm_eps)


def decays(c, at):
    out = [jnp.ones_like(c)]
    for j in (1, 2, 3):
        out.append(jnp.where(at >= j, jnp.exp(jnp.where(at >= j, c - back(c, j), 0.0)), 0.0))
    return out


def inverse_rows(k, b, w):
    low = [None]
    for j in (1, 2, 3):
        dots = jnp.sum(k * back(k, j), -1, keepdims=True)
        low.append(b * dots * w[j])
    one, two, three = low[1], low[2], low[3]
    t1 = -one
    t2 = one * back(one, 1) - two
    t3 = one * back(two, 1) + two * back(one, 2) - three - one * back(one, 1) * back(one, 2)
    return t1, t2, t3


def mixed(x, coefs):
    out = x
    for j, coef in enumerate(coefs):
        out = out + coef * back(x, j + 1)
    return out


def dot(a, b):
    return jnp.dot(a, b, preferred_element_type=F32)


def columns_of(rows):
    eye = (
        lax.broadcasted_iota(jnp.int32, (OWN, 128), 0)
        == lax.broadcasted_iota(jnp.int32, (OWN, 128), 1)
    ).astype(F32)
    return lax.dot_general(
        eye, rows, (((1,), (1,)), ((), ())), precision=HIGHEST, preferred_element_type=F32
    )


def pick(cols, at):
    lane = lax.broadcasted_iota(jnp.int32, cols.shape, 1)
    return wide(jnp.sum(jnp.where(lane == at, cols, 0.0), -1, keepdims=True), 128)


def both(x):
    return jnp.concatenate([x, x], 1)


def commit_kernel(small_ref, rate_ref, keys_ref, values_ref, state_ref, out_ref, lhs, ktail, bv, tri, last):
    step = pl.program_id(0)

    @pl.when(step == 0)
    def _():
        at = place((OWN, 128))
        s = small_ref[...]
        row = lax.broadcasted_iota(jnp.int32, (8, 128), 0)
        rate = jnp.zeros((8, 128), F32)
        for h in range(HD):
            rate = jnp.where(row == 4 + h, rate_ref[h], rate)
        taken = s[8:16]
        top = jnp.where(row < 4, sigmoid(s[0:8]), -rate * softplus(s[0:8])) * taken
        cols = columns_of(jnp.concatenate([top, taken], 0))
        for h in range(HD):
            b = wide(cols[:, h : h + 1], 128)
            g = wide(cols[:, 4 + h : 5 + h], 128)
            k = unit(keys_ref[:, h * DK : (h + 1) * DK].astype(F32))
            c = running_sum(g, at)
            tail = tail_sum(g, at)
            w = decays(c, at)
            t1, t2, t3 = inverse_rows(k, b, w)
            tri[h, 0], tri[h, 1], tri[h, 2] = t1, t2, t3
            lhs[h] = b * k * jnp.exp(c)
            ktail[h] = k * jnp.exp(tail)
            bv[h] = both(b) * values_ref[:, h * DV : (h + 1) * DV].astype(F32)
            last[h] = jnp.exp(c + tail)

    rows = pl.ds(pl.multiple_of(step * 8, 8), 8)
    row = lax.broadcasted_iota(jnp.int32, (8, 256), 0)
    row1 = lax.broadcasted_iota(jnp.int32, (8, 128), 0)
    for h in range(HD):
        left = lhs[h, rows, :].astype(BF16)
        s0, s1 = state_ref[0, h], state_ref[1, h]
        z = jnp.where(row < 4, dot(left, s0.astype(BF16)), dot(left, s1.astype(BF16)))
        coefs = [both(tri[h, j, rows, :]) for j in range(3)]
        fresh = mixed(bv[h, rows, :] - z, coefs)
        kt = ktail[h, rows, :]
        kt2 = jnp.concatenate([jnp.where(row1 < 4, kt, 0.0), jnp.where(row1 >= 4, kt, 0.0)], 1)
        upd = lax.dot_general(
            kt2.astype(BF16),
            fresh.astype(BF16),
            (((0,), (0,)), ((), ())),
            preferred_element_type=F32,
        )
        keep = last[h, rows, :]
        out_ref[0, h] = s0 * keep[0:1, 0:1] + upd[0:DK]
        out_ref[1, h] = s1 * keep[4:5, 0:1] + upd[DK:]


def commit(small, rate, keys, values, state):
    whole = lambda *shape: pl.BlockSpec(shape, lambda i: (0,) * len(shape))
    return pl.pallas_call(
        commit_kernel,
        grid=(SEQ // 2,),
        in_specs=[
            whole(16, 128),
            pl.BlockSpec(memory_space=pltpu.SMEM),
            whole(OWN, HD * DK),
            whole(OWN, HD * DV),
            pl.BlockSpec((2, HD, DK, DV), lambda i: (i, 0, 0, 0)),
        ],
        out_specs=pl.BlockSpec((2, HD, DK, DV), lambda i: (i, 0, 0, 0)),
        out_shape=jax.ShapeDtypeStruct((SEQ, HD, DK, DV), F32),
        scratch_shapes=[
            pltpu.VMEM((HD, OWN, 128), F32),
            pltpu.VMEM((HD, OWN, 128), F32),
            pltpu.VMEM((HD, OWN, DV), F32),
            pltpu.VMEM((HD, 3, OWN, 128), F32),
            pltpu.VMEM((HD, OWN, 128), F32),
        ],
        compiler_params=pltpu.CompilerParams(dimension_semantics=("arbitrary",)),
        name="commit",
    )(small, rate, keys, values, state)


class Sems:
    def __init__(self, send, recv):
        self.send, self.recv, self.at = send, recv, 0
        self.sent = []

    def copy(self, src, dst, device):
        n = self.at
        self.at += 1
        return pltpu.make_async_remote_copy(
            src_ref=src,
            dst_ref=dst,
            send_sem=self.send.at[n],
            recv_sem=self.recv.at[n],
            device_id=device,
            device_id_type=MESH,
        )

    def go(self, copy):
        copy.start()
        self.sent.append(copy)


N_SEM = 3 * 2 + 3 * 5 + 3 * 2 + 3 + 3 + 3 + 12 + 12 + 36 + 7
N_LOC = 8


def mix_kernel(
    hidden,
    gain,
    w_query,
    w_key,
    w_value,
    w_gate,
    w_small,
    w_out,
    rate_ref,
    head_gain,
    state,
    out_ref,
    hid,
    scaled,
    wbuf,
    wsm,
    st32,
    st16,
    wo,
    psend,
    precv,
    ssend,
    srecv,
    csend,
    proj,
    gath,
    osend,
    orecv,
    zk_ref,
    zq_ref,
    lhs_ref,
    send,
    recv,
    loc,
):
    kv, tp = lax.axis_index("kv"), lax.axis_index("tp")
    core, y = lax.rem(tp, 2), tp // 2
    z, x = kv // 4, lax.rem(kv, 4)
    a = z + core * (x - z)
    b = x + core * (z - x)
    sa, sb = 4 - 3 * core, 1 + 3 * core

    def kv_at(a_, b_):
        return a_ * sa + b_ * sb

    def turn(i, d):
        return lax.rem(i + d + 4, 4)

    sems = Sems(send, recv)
    head_block = pl.multiple_of(a * DK, 128)

    own_rows = pl.ds(pl.multiple_of(a * KB, 256), KB)
    local = [
        pltpu.make_async_copy(hidden, hid.at[a], loc.at[0]),
        pltpu.make_async_copy(w_small, wsm.at[a], loc.at[1]),
        pltpu.make_async_copy(w_query.at[:, pl.ds(head_block, DK)], wbuf.at[own_rows, pl.ds(0, DK)], loc.at[2]),
        pltpu.make_async_copy(w_key.at[:, pl.ds(head_block, DK)], wbuf.at[own_rows, pl.ds(DK, DK)], loc.at[3]),
        pltpu.make_async_copy(
            w_value.at[:, pl.ds(pl.multiple_of(a * DV, 256), DV)], wbuf.at[own_rows, pl.ds(2 * DK, DV)], loc.at[4]
        ),
        pltpu.make_async_copy(
            w_gate.at[:, pl.ds(pl.multiple_of(a * DV, 256), DV)],
            wbuf.at[own_rows, pl.ds(2 * DK + DV, DV)],
            loc.at[5],
        ),
        pltpu.make_async_copy(state, st32, loc.at[6]),
        pltpu.make_async_copy(w_out, wo, loc.at[7]),
    ]
    for copy in local:
        copy.start()

    barrier = pltpu.get_barrier_semaphore()
    for d in (1, 2, 3):
        pl.semaphore_signal(barrier, inc=1, device_id=(kv_at(turn(a, d), b), tp), device_id_type=MESH)
        pl.semaphore_signal(barrier, inc=1, device_id=(kv_at(a, turn(b, d)), tp), device_id_type=MESH)
    for e in range(1, 8):
        pl.semaphore_signal(barrier, inc=1, device_id=(kv, lax.rem(tp + e, 8)), device_id_type=MESH)
    pl.semaphore_wait(barrier, 13)

    def quarter(i):
        return pl.ds(pl.multiple_of(i * 256, 256), 256)

    hid_in = {}
    for d in (2, 1, 3):
        peer = (kv_at(turn(a, d), b), tp)
        for e in (0, 2):
            rows = quarter(turn(y, e))
            copy = sems.copy(hidden.at[rows, :], hid.at[a, rows, :], peer)
            sems.go(copy)
            hid_in[d, e] = copy
    w_in = {}
    for d in (2, 1, 3):
        to = turn(a, d)
        peer = (kv_at(to, b), tp)
        cols = pl.ds(pl.multiple_of(to * DK, 128), DK)
        cols2 = pl.ds(pl.multiple_of(to * DV, 256), DV)
        w_in[d] = [
            sems.copy(w_query.at[:, cols], wbuf.at[own_rows, pl.ds(0, DK)], peer),
            sems.copy(w_key.at[:, cols], wbuf.at[own_rows, pl.ds(DK, DK)], peer),
            sems.copy(w_value.at[:, cols2], wbuf.at[own_rows, pl.ds(2 * DK, DV)], peer),
            sems.copy(w_gate.at[:, cols2], wbuf.at[own_rows, pl.ds(2 * DK + DV, DV)], peer),
            sems.copy(w_small, wsm.at[a], peer),
        ]
        for copy in w_in[d]:
            sems.go(copy)

    def scale_block(slot):
        weight = gain[kv_at(slot, b)]

        def body(n, _):
            kb, ka = n // 4, lax.rem(n, 4)
            rows = pl.ds(pl.multiple_of(kv_at(ka, kb) * OWN, OWN), OWN)
            to = pl.ds(pl.multiple_of(n * OWN, OWN), OWN)
            block = hid[slot, rows, :].astype(F32) * weight
            scaled[to, pl.ds(pl.multiple_of(slot * KB, 256), KB)] = block.astype(BF16)
            return 0

        lax.fori_loop(0, 16, body, 0)

    local[0].wait()
    scale_block(a)
    y_in = {}
    for d in (1, 3, 2):
        hid_in[d, 0].wait_recv()
        slot = turn(a, -d)
        rows = quarter(y)
        y_in[d] = []
        for e in (1, 3):
            peer = (kv, 2 * turn(y, e) + core)
            copy = sems.copy(hid.at[slot, rows, :], hid.at[slot, rows, :], peer)
            sems.go(copy)
            y_in[d].append(copy)

    local[6].wait()

    def round_states(n, _):
        st16[n] = st32[n].astype(BF16)
        return 0

    lax.fori_loop(0, SEQ, round_states, 0)

    for d in (1, 3, 2):
        hid_in[d, 2].wait_recv()
        for copy in y_in[d]:
            copy.wait_recv()
        scale_block(turn(a, -d))

    for n in (1, 2, 3, 4, 5):
        local[n].wait()
    for d in (1, 3, 2):
        for copy in w_in[d]:
            copy.wait_recv()

    weights = wbuf[...]
    ones = jnp.ones((8, 4 * KB), BF16)
    small_w = jnp.concatenate([wsm[i] for i in range(4)], 1).astype(BF16)
    s_in, p_in = {}, {}
    for d in (2, 1, 3, 0):
        to = turn(b, d)
        peer = (kv_at(a, to), tp)
        rows = pl.ds(pl.multiple_of(to * 256, 256), 256)
        psend[d] = dot(scaled[rows, :], weights).astype(BF16)
        if d:
            copy = sems.copy(psend.at[d], precv.at[d - 1], peer)
            sems.go(copy)
            p_in[d] = copy
    for d in (2, 1, 3, 0):
        to = turn(b, d)
        peer = (kv_at(a, to), tp)
        mine = pl.ds(pl.multiple_of(to * 256 + a * OWN, OWN), OWN)
        token = pl.ds(pl.multiple_of(kv_at(a, to) * OWN, OWN), OWN)
        nt = (((1,), (1,)), ((), ()))
        part = lax.dot_general(small_w, scaled[mine, :], nt, preferred_element_type=F32)
        square = jnp.zeros((8, OWN), F32)
        for i in range(4):
            h32 = hid[i, token, :].astype(F32)
            sq = h32 * h32
            high = sq.astype(BF16)
            low = (sq - high.astype(F32)).astype(BF16)
            square = square + lax.dot_general(ones[:, :KB], high, nt, preferred_element_type=F32)
            square = square + lax.dot_general(ones[:, :KB], low, nt, preferred_element_type=F32)
        ssend[d] = jnp.concatenate([jnp.concatenate([part, square], 0), jnp.zeros((16, 64), F32)], 1)
        if d:
            copy = sems.copy(ssend.at[d], srecv.at[d - 1], peer)
            sems.go(copy)
            s_in[d] = copy

    for d in (1, 3, 2):
        p_in[d].wait_recv()
    c_in = {}
    for d in (2, 1, 3, 0):
        to = turn(a, d)
        rows = pl.ds(pl.multiple_of(to * OWN, OWN), OWN)
        total = psend[0, rows, :].astype(F32)
        for i in range(3):
            total = total + precv[i, rows, :].astype(F32)
        if d:
            csend[d - 1] = total.astype(BF16)
            copy = sems.copy(csend.at[d - 1], proj.at[a], (kv_at(to, b), tp))
            sems.go(copy)
            c_in[d] = copy
        else:
            proj[a] = total.astype(BF16)

    for d in (1, 3, 2):
        s_in[d].wait_recv()
    small = ssend[0]
    for i in range(3):
        small = small + srecv[i]
    inv = lax.rsqrt(small[8:16] / D + norm_eps)
    row = lax.broadcasted_iota(jnp.int32, (8, 128), 0)
    rate = jnp.zeros((8, 128), F32)
    for h in range(HD):
        rate = jnp.where(row == 4 + h, rate_ref[h], rate)
    pre = small[0:8] * inv
    top = jnp.where(row < 4, sigmoid(pre), -rate * softplus(pre))
    cols = columns_of(jnp.concatenate([top, inv], 0))
    inv_col = cols[:, 8:9]
    at = place((OWN, 128))
    row4 = lax.broadcasted_iota(jnp.int32, (8, DV), 0)

    first_in, peer_in = {}, {}
    for d in range(4):
        h = turn(a, -d)
        if d:
            c_in[d].wait_recv()
        bcol = pick(cols, h)
        c = running_sum(pick(cols, h + 4), at)
        w = decays(c, at)
        grow = jnp.exp(c)
        q = unit(silu(proj[h, :, 0:DK].astype(F32) * inv_col)) * DK ** (-0.5)
        k = unit(silu(proj[h, :, DK : 2 * DK].astype(F32) * inv_col))
        v = silu(proj[h, :, 2 * DK : 2 * DK + DV].astype(F32) * inv_col)
        coefs = [both(t) for t in inverse_rows(k, bcol, w)]
        scores = [both(wide(jnp.sum(q * back(k, j), -1, keepdims=True), 128) * w[j]) for j in range(4)]
        kl = bcol * k * grow
        ql = q * grow
        for i in range(SEQ // 2):
            rows = slice(8 * i, 8 * i + 8)
            left = jnp.concatenate([kl[rows], ql[rows]], 0).astype(BF16)
            z0 = dot(left, st16[2 * i, h])
            z1 = dot(left, st16[2 * i + 1, h])
            zk_ref[rows, :] = jnp.where(row4 < 4, z0[0:8], z1[0:8])
            zq_ref[rows, :] = jnp.where(row4 < 4, z0[8:16], z1[8:16])
        fresh = mixed(both(bcol) * v - zk_ref[...], coefs)
        res = zq_ref[...]
        for j in range(4):
            res = res + scores[j] * back(fresh, j)
        norm = res * lax.rsqrt(jnp.mean(res * res, -1, keepdims=True) + norm_eps) * head_gain[...]
        gate = silu(proj[h, :, 2 * DK + DV :].astype(F32) * inv_col)
        gath[kv, h] = (norm * gate).astype(BF16)
        for e in (2, 1, 3):
            copy = sems.copy(gath.at[kv, h], gath.at[kv, h], (kv_at(a, turn(b, e)), tp))
            sems.go(copy)
            peer_in[e, d] = copy
            copy = sems.copy(gath.at[kv, h], gath.at[kv, h], (kv_at(turn(a, e), b), tp))
            sems.go(copy)
            first_in[e, d] = copy

    on_in = []
    for d in range(4):
        for e in (1, 3, 2):
            first_in[e, d].wait_recv()
            src = turn(a, -e)
            h = turn(src, -d)
            block = gath.at[kv_at(src, b), h]
            for f in (2, 1, 3):
                copy = sems.copy(block, block, (kv_at(a, turn(b, f)), tp))
                sems.go(copy)
                on_in.append(copy)
    for copy in peer_in.values():
        copy.wait_recv()
    for copy in on_in:
        copy.wait_recv()

    local[7].wait()
    o_in = {}
    for e in (4, 5, 2, 3, 6, 7, 1, 0):
        to = lax.rem(tp + e, 8)
        total = None
        for h in range(HD):
            part = jnp.concatenate([gath[2 * to, h], gath[2 * to + 1, h]], 0)
            term = dot(part, wo[h * DV : (h + 1) * DV, :])
            total = term if total is None else total + term
        osend[e] = total.astype(BF16)
        if e:
            copy = sems.copy(osend.at[e], orecv.at[e - 1], (kv, to))
            sems.go(copy)
            o_in[e] = copy
    for e in range(1, 8):
        o_in[e].wait_recv()
    total = osend[0].astype(F32)
    for i in range(7):
        total = total + orecv[i].astype(F32)
    out_ref[...] = total.astype(BF16)
    for copy in sems.sent:
        copy.wait_send()
    assert sems.at == N_SEM, sems.at


def mix(hidden, gain, w_query, w_key, w_value, w_gate, w_small, w_out, rate, head_gain, state):
    hbm = pl.BlockSpec(memory_space=pl.ANY)
    vmem = pl.BlockSpec(memory_space=pltpu.VMEM)
    return pl.pallas_call(
        mix_kernel,
        in_specs=[hbm, vmem, hbm, hbm, hbm, hbm, hbm, hbm, pl.BlockSpec(memory_space=pltpu.SMEM), vmem, hbm],
        out_specs=vmem,
        out_shape=jax.ShapeDtypeStruct((128, 256), BF16),
        scratch_shapes=[
            pltpu.VMEM((4, TOK, KB), BF16),
            pltpu.VMEM((TOK, 4 * KB), BF16),
            pltpu.VMEM((4 * KB, COLS), BF16),
            pltpu.VMEM((4, 8, KB), F32),
            pltpu.VMEM((SEQ, HD, DK, DV), F32),
            pltpu.VMEM((SEQ, HD, DK, DV), BF16),
            pltpu.VMEM((HD * DV, 256), BF16),
            pltpu.VMEM((4, 256, COLS), BF16),
            pltpu.VMEM((3, 256, COLS), BF16),
            pltpu.VMEM((4, 16, 128), F32),
            pltpu.VMEM((3, 16, 128), F32),
            pltpu.VMEM((3, OWN, COLS), BF16),
            pltpu.VMEM((HD, OWN, COLS), BF16),
            pltpu.VMEM((16, HD, OWN, DV), BF16),
            pltpu.VMEM((8, 128, 256), BF16),
            pltpu.VMEM((7, 128, 256), BF16),
            pltpu.VMEM((OWN, DV), F32),
            pltpu.VMEM((OWN, DV), F32),
            pltpu.VMEM((OWN, DK), F32),
            pltpu.SemaphoreType.DMA((N_SEM,)),
            pltpu.SemaphoreType.DMA((N_SEM,)),
            pltpu.SemaphoreType.DMA((N_LOC,)),
        ],
        compiler_params=pltpu.CompilerParams(
            collective_id=0, has_side_effects=True, vmem_limit_bytes=60 * 1024 * 1024
        ),
        name="mix",
    )(hidden, gain, w_query, w_key, w_value, w_gate, w_small, w_out, rate, head_gain, state)


def per_device(
    hidden,
    norm_gain,
    w_query,
    w_key,
    w_value,
    w_gate,
    w_write,
    w_decay,
    w_out,
    decay_rate,
    head_gain,
    carried_state,
    last_keys,
    last_values,
    last_writes,
    last_decays,
    accepted,
):
    def rows_of(small):
        return jnp.transpose(small, (2, 0, 1)).reshape(HD, OWN)

    taken = (jnp.arange(4, dtype=jnp.int32)[None, :] < accepted[:, None]).astype(F32).reshape(1, OWN)
    small = jnp.concatenate(
        [rows_of(last_writes), rows_of(last_decays), jnp.broadcast_to(taken, (8, OWN))], 0
    )
    small = jnp.pad(small, ((0, 0), (0, 128 - OWN)))
    committed = commit(
        small,
        decay_rate,
        last_keys.reshape(OWN, HD * DK),
        last_values.reshape(OWN, HD * DV),
        carried_state,
    )
    w_small = jnp.concatenate([w_write.T, w_decay.T], 0).astype(F32)
    mixed_out = mix(
        hidden,
        norm_gain.astype(F32).reshape(16, 1, 256),
        w_query,
        w_key,
        w_value,
        w_gate,
        w_small,
        w_out,
        decay_rate,
        head_gain.reshape(1, DV),
        committed,
    )
    return (mixed_out, committed)


def solution(mesh):
    return jax.shard_map(
        per_device,
        mesh=mesh,
        in_specs=(
            P(None, "kv"),
            P(),
            P("kv", "tp"),
            P("kv", "tp"),
            P("kv", "tp"),
            P("kv", "tp"),
            P("kv", "tp"),
            P("kv", "tp"),
            P("tp", "kv"),
            P("tp"),
            P(),
            P("kv", "tp", None, None),
            P("kv", None, "tp"),
            P("kv", None, "tp"),
            P("kv", None, "tp"),
            P("kv", None, "tp"),
            P("kv"),
        ),
        out_specs=(P("tp", "kv"), P("kv", "tp", None, None)),
        check_vma=False,
    )
```

```python
import functools

import jax
import jax.numpy as jnp
from jax import lax
from jax.experimental import pallas as pl
from jax.experimental.pallas import tpu as pltpu
from jax.sharding import PartitionSpec as P

MESH = pl.DeviceIdType.MESH
HIGHEST = lax.Precision.HIGHEST
F32 = jnp.float32
BF16 = jnp.bfloat16
norm_eps = 1e-06

TOK = 1024
OWN = 64
SEQ = 16
HD = 4
DK = 128
DV = 256
KB = 256
D = 4096
COLS = 2 * DK + 2 * DV


def softplus(x):
    return jnp.maximum(x, 0.0) + jnp.log1p(jnp.exp(-jnp.abs(x)))


def sigmoid(x):
    return 1.0 / (1.0 + jnp.exp(-x))


def silu(x):
    return x * sigmoid(x)


def place(shape):
    return lax.rem(lax.broadcasted_iota(jnp.int32, shape, 0), 4)


def back(x, j):
    return x if j == 0 else pltpu.roll(x, j, 0)


def ahead(x, j):
    return pltpu.roll(x, x.shape[0] - j, 0)


def wide(col, width):
    return jnp.broadcast_to(col, (col.shape[0], width))


def running_sum(g, at):
    c = g
    for j in (1, 2, 3):
        c = c + jnp.where(at >= j, back(g, j), 0.0)
    return c


def tail_sum(g, at):
    s = jnp.zeros_like(g)
    for j in (1, 2, 3):
        s = s + jnp.where(at + j <= 3, ahead(g, j), 0.0)
    return s


def unit(x):
    return x * lax.rsqrt(jnp.sum(x * x, -1, keepdims=True) + norm_eps)


def decays(c, at):
    out = [jnp.ones_like(c)]
    for j in (1, 2, 3):
        out.append(jnp.where(at >= j, jnp.exp(jnp.where(at >= j, c - back(c, j), 0.0)), 0.0))
    return out


def inverse_rows(k, b, w):
    low = [None]
    for j in (1, 2, 3):
        dots = jnp.sum(k * back(k, j), -1, keepdims=True)
        low.append(b * dots * w[j])
    one, two, three = low[1], low[2], low[3]
    t1 = -one
    t2 = one * back(one, 1) - two
    t3 = one * back(two, 1) + two * back(one, 2) - three - one * back(one, 1) * back(one, 2)
    return t1, t2, t3


def mixed(x, coefs):
    out = x
    for j, coef in enumerate(coefs):
        out = out + coef * back(x, j + 1)
    return out


def dot(a, b):
    return jnp.dot(a, b, preferred_element_type=F32)


def columns_of(rows):
    eye = (
        lax.broadcasted_iota(jnp.int32, (OWN, 128), 0)
        == lax.broadcasted_iota(jnp.int32, (OWN, 128), 1)
    ).astype(F32)
    return lax.dot_general(
        eye, rows, (((1,), (1,)), ((), ())), precision=HIGHEST, preferred_element_type=F32
    )


def pick(cols, at):
    lane = lax.broadcasted_iota(jnp.int32, cols.shape, 1)
    return wide(jnp.sum(jnp.where(lane == at, cols, 0.0), -1, keepdims=True), 128)


def both(x):
    return jnp.concatenate([x, x], 1)


class Sems:
    def __init__(self, send, recv):
        self.send, self.recv, self.at = send, recv, 0
        self.sent = []

    def go(self, src, dst, device):
        n = self.at
        self.at += 1
        copy = pltpu.make_async_remote_copy(
            src_ref=src,
            dst_ref=dst,
            send_sem=self.send.at[n],
            recv_sem=self.recv.at[n],
            device_id=device,
            device_id_type=MESH,
        )
        copy.start()
        self.sent.append(copy)
        return copy


N_SEM = 6 + 3 * 6 + 6 + 9 + 3 + 9 + 12 + 12 + 36
NT = (((1,), (1,)), ((), ()))


def kernel(
    hidden,
    gain,
    w_query,
    w_key,
    w_value,
    w_gate,
    w_write,
    w_decay,
    w_out,
    rate_ref,
    head_gain,
    state,
    last_keys,
    last_values,
    last_writes,
    last_decays,
    accepted,
    out_ref,
    st32,
    hid,
    scaled,
    wbuf,
    wsm,
    st16,
    wo,
    lhs,
    ktail,
    bv,
    tri,
    last,
    psend,
    precv,
    ssend,
    srecv,
    csend,
    proj,
    coef,
    zk,
    zq,
    gath,
    osend,
    orecv,
    send,
    recv,
    loc,
    o_send,
    o_recv,
):
    kv, tp = lax.axis_index("kv"), lax.axis_index("tp")
    core, y = lax.rem(tp, 2), tp // 2
    z, x = kv // 4, lax.rem(kv, 4)
    a = z + core * (x - z)
    b = x + core * (z - x)
    sa, sb = 4 - 3 * core, 1 + 3 * core

    def kv_at(a_, b_):
        return a_ * sa + b_ * sb

    def turn(i, d):
        return lax.rem(i + d + 4, 4)

    def head_cols(h, width):
        return pl.ds(pl.multiple_of(h * width, width), width)

    sems = Sems(send, recv)
    own_rows = pl.ds(pl.multiple_of(a * KB, 256), KB)

    def weight_parts(h):
        return [
            (w_query.at[:, head_cols(h, DK)], wbuf.at[0, own_rows, pl.ds(0, DK)]),
            (w_key.at[:, head_cols(h, DK)], wbuf.at[0, own_rows, pl.ds(DK, DK)]),
            (w_write, wsm.at[a, 0]),
            (w_decay, wsm.at[a, 1]),
            (w_value.at[:, head_cols(h, DV)], wbuf.at[1, own_rows, :]),
            (w_gate.at[:, head_cols(h, DV)], wbuf.at[2, own_rows, :]),
        ]

    pairs = [(hidden, hid.at[a]), (state, st32), (w_out, wo)] + weight_parts(a)
    local = [pltpu.make_async_copy(src, dst, loc.at[n]) for n, (src, dst) in enumerate(pairs)]
    for copy in local:
        copy.start()

    barrier = pltpu.get_barrier_semaphore()
    for d in (1, 2, 3):
        pl.semaphore_signal(barrier, inc=1, device_id=(kv_at(turn(a, d), b), tp), device_id_type=MESH)
        pl.semaphore_signal(barrier, inc=1, device_id=(kv_at(a, turn(b, d)), tp), device_id_type=MESH)
    for e in range(1, 8):
        pl.semaphore_signal(barrier, inc=1, device_id=(kv, lax.rem(tp + e, 8)), device_id_type=MESH)
    pl.semaphore_wait(barrier, 13)

    def quarter(i):
        return pl.ds(pl.multiple_of(i * 256, 256), 256)

    hid_in = {}
    for e in (0, 2):
        for d in (1, 3, 2):
            rows = quarter(turn(y, e))
            hid_in[d, e] = sems.go(hidden.at[rows, :], hid.at[a, rows, :], (kv_at(turn(a, d), b), tp))
    w_in = {d: [] for d in (1, 2, 3)}
    for first, past in ((0, 4), (4, 5), (5, 6)):
        for d in (2, 1, 3):
            to = turn(a, d)
            for src, dst in weight_parts(to)[first:past]:
                w_in[d].append(sems.go(src, dst, (kv_at(to, b), tp)))

    at = place((OWN, 128))
    which = lax.broadcasted_iota(jnp.int32, (OWN, SEQ), 0)
    seq = lax.broadcasted_iota(jnp.int32, (OWN, SEQ), 1)
    raw = jnp.zeros((OWN, 8), F32)
    for p in range(4):
        raw = raw + lax.dot_general(
            (which == 4 * seq + p).astype(F32),
            jnp.concatenate([last_writes[p], last_decays[p]], 0),
            NT,
            precision=HIGHEST,
            preferred_element_type=F32,
        )
    count = jnp.sum(jnp.where(which // 4 == seq, accepted[...].astype(F32), 0.0), -1, keepdims=True)
    taken = (place((OWN, 8)).astype(F32) < count).astype(F32)
    lane8 = lax.broadcasted_iota(jnp.int32, (OWN, 8), 1)
    rate = jnp.zeros((OWN, 8), F32)
    for h in range(HD):
        rate = jnp.where(lane8 == 4 + h, rate_ref[h], rate)
    cols = jnp.where(lane8 < 4, sigmoid(raw), -rate * softplus(raw)) * taken

    for n in range(SEQ // 2):
        rows = slice(8 * n, 8 * n + 8)
        lhs_pair = [last_keys[2 * n + i].astype(F32) for i in (0, 1)]
        val_pair = [last_values[2 * n + i].astype(F32) for i in (0, 1)]
        for h in range(HD):
            cut = slice(h * DK, (h + 1) * DK)
            lhs[h, rows, :] = jnp.concatenate([v[:, cut] for v in lhs_pair], 0)
            cut = slice(h * DV, (h + 1) * DV)
            bv[h, rows, :] = jnp.concatenate([v[:, cut] for v in val_pair], 0)

    def old_head(h, _):
        bcol, g = pick(cols, h), pick(cols, h + 4)
        k = unit(lhs[h])
        c = running_sum(g, at)
        tail = tail_sum(g, at)
        t1, t2, t3 = inverse_rows(k, bcol, decays(c, at))
        tri[h, 0], tri[h, 1], tri[h, 2] = t1, t2, t3
        lhs[h] = bcol * k * jnp.exp(c)
        ktail[h] = k * jnp.exp(tail)
        bv[h] = both(bcol) * bv[h]
        last[h] = jnp.exp(c + tail)
        return 0

    lax.fori_loop(0, HD, old_head, 0)

    y_in = {}
    for d in (1, 3, 2):
        hid_in[d, 0].wait_recv()
        slot = turn(a, -d)
        rows = quarter(y)
        y_in[d] = [
            sems.go(hid.at[slot, rows, :], hid.at[slot, rows, :], (kv, 2 * turn(y, e) + core)) for e in (1, 3)
        ]

    local[1].wait()
    row8 = lax.broadcasted_iota(jnp.int32, (8, DV), 0)
    row8k = lax.broadcasted_iota(jnp.int32, (8, DK), 0)

    def old_pair(n, _):
        rows = pl.ds(pl.multiple_of(n * 8, 8), 8)
        for h in range(HD):
            left = lhs[h, rows, :].astype(BF16)
            s0, s1 = st32[2 * n, h], st32[2 * n + 1, h]
            zz = jnp.where(row8 < 4, dot(left, s0.astype(BF16)), dot(left, s1.astype(BF16)))
            fresh = mixed(bv[h, rows, :] - zz, [both(tri[h, j, rows, :]) for j in range(3)])
            kt = ktail[h, rows, :]
            kt2 = jnp.concatenate([jnp.where(row8k < 4, kt, 0.0), jnp.where(row8k >= 4, kt, 0.0)], 1)
            upd = lax.dot_general(
                kt2.astype(BF16), fresh.astype(BF16), (((0,), (0,)), ((), ())), preferred_element_type=F32
            )
            keep = last[h, rows, :]
            n0 = s0 * keep[0:1, 0:1] + upd[0:DK]
            n1 = s1 * keep[4:5, 0:1] + upd[DK:]
            st32[2 * n, h], st32[2 * n + 1, h] = n0, n1
            st16[2 * n, h], st16[2 * n + 1, h] = n0.astype(BF16), n1.astype(BF16)
        return 0

    lax.fori_loop(0, SEQ // 2, old_pair, 0)

    def scale_block(slot):
        weight = gain[kv_at(slot, b)]

        def body(n, _):
            kb, ka = n // 4, lax.rem(n, 4)
            rows = pl.ds(pl.multiple_of(kv_at(ka, kb) * OWN, OWN), OWN)
            to = pl.ds(pl.multiple_of(n * OWN, OWN), OWN)
            block = hid[slot, rows, :].astype(F32) * weight
            scaled[to, pl.ds(pl.multiple_of(slot * KB, 256), KB)] = block.astype(BF16)
            return 0

        lax.fori_loop(0, 16, body, 0)

    local[0].wait()
    scale_block(a)
    for d in (1, 3, 2):
        hid_in[d, 2].wait_recv()
        for copy in y_in[d]:
            copy.wait_recv()
        scale_block(turn(a, -d))

    p_in, c_in = {}, {}

    def send_parts(chunk, first, past):
        for copy in local[3 + first : 3 + past]:
            copy.wait()
        for d in (1, 3, 2):
            for copy in w_in[d][first:past]:
                copy.wait_recv()
        weights = wbuf[chunk]
        for d in (2, 1, 3, 0):
            to = turn(b, d)
            psend[chunk, d] = dot(scaled[quarter(to), :], weights).astype(BF16)
            if d:
                p_in[chunk, d] = sems.go(
                    psend.at[chunk, d], precv.at[chunk, d - 1], (kv_at(a, to), tp)
                )

    def send_sums(chunk):
        for d in (1, 3, 2):
            p_in[chunk, d].wait_recv()
        for d in (2, 1, 3, 0):
            to = turn(a, d)
            rows = pl.ds(pl.multiple_of(to * OWN, OWN), OWN)
            total = psend[chunk, 0, rows, :].astype(F32)
            for i in range(3):
                total = total + precv[chunk, i, rows, :].astype(F32)
            if d:
                csend[chunk, d - 1] = total.astype(BF16)
                c_in[chunk, d] = sems.go(csend.at[chunk, d - 1], proj.at[chunk, a], (kv_at(to, b), tp))
            else:
                proj[chunk, a] = total.astype(BF16)

    send_parts(0, 0, 4)
    s_in = {}
    ones = jnp.ones((8, KB), BF16)
    for d in (2, 1, 3, 0):
        to = turn(b, d)
        token = pl.ds(pl.multiple_of(kv_at(a, to) * OWN, OWN), OWN)
        mine = pl.ds(pl.multiple_of(to * 256 + a * OWN, OWN), OWN)
        write, decay = jnp.zeros((4, OWN), F32), jnp.zeros((4, OWN), F32)
        square = jnp.zeros((8, OWN), F32)
        for i in range(4):
            rows_i = scaled[mine, i * KB : (i + 1) * KB]
            write = write + lax.dot_general(wsm[i, 0], rows_i, NT, preferred_element_type=F32)
            decay = decay + lax.dot_general(wsm[i, 1], rows_i, NT, preferred_element_type=F32)
            h32 = hid[i, token, :].astype(F32)
            sq = h32 * h32
            high = sq.astype(BF16)
            low = (sq - high.astype(F32)).astype(BF16)
            square = square + lax.dot_general(ones, high, NT, preferred_element_type=F32)
            square = square + lax.dot_general(ones, low, NT, preferred_element_type=F32)
        part = jnp.concatenate([write, decay, square], 0)
        ssend[d] = jnp.concatenate([part, jnp.zeros((16, 64), F32)], 1)
        if d:
            s_in[d] = sems.go(ssend.at[d], srecv.at[d - 1], (kv_at(a, to), tp))
    send_parts(1, 4, 5)
    send_sums(0)
    send_parts(2, 5, 6)

    for d in (1, 3, 2):
        s_in[d].wait_recv()
    small = ssend[0]
    for i in range(3):
        small = small + srecv[i]
    inv = lax.rsqrt(small[8:16] / D + norm_eps)
    row = lax.broadcasted_iota(jnp.int32, (8, 128), 0)
    rate = jnp.zeros((8, 128), F32)
    for h in range(HD):
        rate = jnp.where(row == 4 + h, rate_ref[h], rate)
    pre = small[0:8] * inv
    top = jnp.where(row < 4, sigmoid(pre), -rate * softplus(pre))
    cols = columns_of(jnp.concatenate([top, inv], 0))
    inv_col = cols[:, 8:9]
    send_sums(1)

    def new_keys(d):
        h = turn(a, -d)
        if d:
            c_in[0, d].wait_recv()
        bcol = pick(cols, h)
        c = running_sum(pick(cols, h + 4), at)
        w = decays(c, at)
        grow = jnp.exp(c)
        q = unit(silu(proj[0, h, :, 0:DK].astype(F32) * inv_col)) * DK ** (-0.5)
        k = unit(silu(proj[0, h, :, DK : 2 * DK].astype(F32) * inv_col))
        kl, ql = bcol * k * grow, q * grow
        for i in range(SEQ // 2):
            rows = slice(8 * i, 8 * i + 8)
            left = jnp.concatenate([kl[rows], ql[rows]], 0).astype(BF16)
            z0 = dot(left, st16[2 * i, h])
            z1 = dot(left, st16[2 * i + 1, h])
            zk[d, rows, :] = jnp.where(row8 < 4, z0[0:8], z1[0:8])
            zq[d, rows, :] = jnp.where(row8 < 4, z0[8:16], z1[8:16])
        t1, t2, t3 = inverse_rows(k, bcol, w)
        coef[d, 0], coef[d, 1], coef[d, 2] = t1, t2, t3
        for j in range(4):
            coef[d, 3 + j] = wide(jnp.sum(q * back(k, j), -1, keepdims=True), 128) * w[j]
        coef[d, 7] = bcol

    new_keys(0)
    new_keys(1)
    send_sums(2)
    new_keys(3)
    new_keys(2)

    first_in, peer_in = {}, {}
    for d in (0, 1, 3, 2):
        h = turn(a, -d)
        if d:
            c_in[1, d].wait_recv()
            c_in[2, d].wait_recv()
        v = silu(proj[1, h].astype(F32) * inv_col)
        fresh = mixed(both(coef[d, 7]) * v - zk[d], [both(coef[d, j]) for j in range(3)])
        res = zq[d]
        for j in range(4):
            res = res + both(coef[d, 3 + j]) * back(fresh, j)
        norm = res * lax.rsqrt(jnp.mean(res * res, -1, keepdims=True) + norm_eps) * head_gain[...]
        gath[kv, h] = (norm * silu(proj[2, h].astype(F32) * inv_col)).astype(BF16)
        block = gath.at[kv, h]
        for e in (2, 1, 3):
            first_in[e, d] = sems.go(block, block, (kv_at(turn(a, e), b), tp))
        for e in (2, 1, 3):
            peer_in[e, d] = sems.go(block, block, (kv_at(a, turn(b, e)), tp))

    on_in = {}
    for d in (0, 1, 3, 2):
        for e in (1, 3, 2):
            first_in[e, d].wait_recv()
            src = turn(a, -e)
            block = gath.at[kv_at(src, b), turn(src, -d)]
            for f in (2, 1, 3):
                on_in[e, f, d] = sems.go(block, block, (kv_at(a, turn(b, f)), tp))

    local[2].wait()
    weights = wo[...]
    outs = []

    def send_out(src, waits):
        n = len(outs)
        for copy in waits:
            copy.wait_recv()
        to, half = src // 2, lax.rem(src, 2)
        e = lax.rem(to - tp + 8, 8)
        rows = pl.ds(pl.multiple_of(half * OWN, OWN), OWN)
        total = dot(jnp.concatenate([gath[src, h] for h in range(HD)], 1), weights).astype(BF16)
        osend[n] = total
        copy = pltpu.make_async_remote_copy(
            src_ref=osend.at[n],
            dst_ref=orecv.at[e, rows, :],
            send_sem=o_send.at[n],
            recv_sem=o_recv.at[2 * e + half],
            device_id=(kv, to),
            device_id_type=MESH,
        )
        outs.append((e, copy))

        @pl.when(e != 0)
        def _():
            copy.start()

        @pl.when(e == 0)
        def _():
            orecv[0, rows, :] = total

    send_out(kv, [])
    for e in (1, 3, 2):
        send_out(kv_at(turn(a, -e), b), [])
    for e in (1, 3, 2):
        send_out(kv_at(a, turn(b, -e)), [peer_in[e, d] for d in range(4)])
    for e in (1, 3, 2):
        for f in (1, 3, 2):
            send_out(kv_at(turn(a, -e), turn(b, -f)), [on_in[e, f, d] for d in range(4)])

    for e in range(1, 8):
        for half in (0, 1):
            rows = pl.ds(half * OWN, OWN)
            pltpu.make_async_remote_copy(
                src_ref=osend.at[0],
                dst_ref=orecv.at[e, rows, :],
                send_sem=o_send.at[0],
                recv_sem=o_recv.at[2 * e + half],
                device_id=(kv, lax.rem(tp + e, 8)),
                device_id_type=MESH,
            ).wait_recv()
    total = orecv[0].astype(F32)
    for i in range(1, 8):
        total = total + orecv[i].astype(F32)
    out_ref[...] = total.astype(BF16)
    for copy in sems.sent:
        copy.wait_send()
    for e, copy in outs:

        @pl.when(e != 0)
        def _():
            copy.wait_send()

    assert sems.at == N_SEM, sems.at


def mix(*args):
    hbm = pl.BlockSpec(memory_space=pl.ANY)
    vmem = pl.BlockSpec(memory_space=pltpu.VMEM)
    smem = pl.BlockSpec(memory_space=pltpu.SMEM)
    return pl.pallas_call(
        kernel,
        in_specs=[hbm, vmem] + [hbm] * 7 + [smem, vmem, hbm] + [vmem] * 5,
        out_specs=(vmem, vmem),
        out_shape=(jax.ShapeDtypeStruct((128, 256), BF16), pltpu.VMEM((SEQ, HD, DK, DV), F32)),
        scratch_shapes=[
            pltpu.VMEM((4, TOK, KB), BF16),
            pltpu.VMEM((TOK, 4 * KB), BF16),
            pltpu.VMEM((3, 4 * KB, 256), BF16),
            pltpu.VMEM((4, 2, 4, KB), BF16),
            pltpu.VMEM((SEQ, HD, DK, DV), BF16),
            pltpu.VMEM((HD * DV, 256), BF16),
            pltpu.VMEM((HD, OWN, 128), F32),
            pltpu.VMEM((HD, OWN, 128), F32),
            pltpu.VMEM((HD, OWN, DV), F32),
            pltpu.VMEM((HD, 3, OWN, 128), F32),
            pltpu.VMEM((HD, OWN, 128), F32),
            pltpu.VMEM((3, 4, 256, 256), BF16),
            pltpu.VMEM((3, 3, 256, 256), BF16),
            pltpu.VMEM((4, 16, 128), F32),
            pltpu.VMEM((3, 16, 128), F32),
            pltpu.VMEM((3, 3, OWN, 256), BF16),
            pltpu.VMEM((3, HD, OWN, 256), BF16),
            pltpu.VMEM((4, 8, OWN, 128), F32),
            pltpu.VMEM((4, OWN, DV), F32),
            pltpu.VMEM((4, OWN, DV), F32),
            pltpu.VMEM((16, HD, OWN, DV), BF16),
            pltpu.VMEM((16, OWN, 256), BF16),
            pltpu.VMEM((8, 128, 256), BF16),
            pltpu.SemaphoreType.DMA((N_SEM,)),
            pltpu.SemaphoreType.DMA((N_SEM,)),
            pltpu.SemaphoreType.DMA((9,)),
            pltpu.SemaphoreType.DMA((16,)),
            pltpu.SemaphoreType.DMA((16,)),
        ],
        compiler_params=pltpu.CompilerParams(
            collective_id=0, has_side_effects=True, vmem_limit_bytes=50 * 1024 * 1024
        ),
        name="mix",
    )(*[pltpu.with_memory_space_constraint(arg, pltpu.HBM) for arg in args])


def per_device(
    hidden,
    norm_gain,
    w_query,
    w_key,
    w_value,
    w_gate,
    w_write,
    w_decay,
    w_out,
    decay_rate,
    head_gain,
    carried_state,
    last_keys,
    last_values,
    last_writes,
    last_decays,
    accepted,
):
    mixed_out, committed = mix(
        hidden,
        norm_gain.astype(F32).reshape(16, 1, 256),
        w_query,
        w_key,
        w_value,
        w_gate,
        w_write.T,
        w_decay.T,
        w_out,
        decay_rate,
        head_gain.reshape(1, DV),
        carried_state,
        last_keys,
        last_values,
        jnp.transpose(last_writes, (1, 2, 0)),
        jnp.transpose(last_decays, (1, 2, 0)),
        accepted.reshape(1, SEQ),
    )
    return (mixed_out, committed)


def solution(mesh):
    return jax.shard_map(
        per_device,
        mesh=mesh,
        in_specs=(
            P(None, "kv"),
            P(),
            P("kv", "tp"),
            P("kv", "tp"),
            P("kv", "tp"),
            P("kv", "tp"),
            P("kv", "tp"),
            P("kv", "tp"),
            P("tp", "kv"),
            P("tp"),
            P(),
            P("kv", "tp", None, None),
            P("kv", None, "tp"),
            P("kv", None, "tp"),
            P("kv", None, "tp"),
            P("kv", None, "tp"),
            P("kv"),
        ),
        out_specs=(P("tp", "kv"), P("kv", "tp", None, None)),
        check_vma=False,
    )
```

```python
import functools

import jax
import jax.numpy as jnp
from jax import lax
from jax.experimental import pallas as pl
from jax.experimental.pallas import tpu as pltpu
from jax.sharding import PartitionSpec as P

MESH = pl.DeviceIdType.MESH
HIGHEST = lax.Precision.HIGHEST
F32 = jnp.float32
BF16 = jnp.bfloat16
norm_eps = 1e-06

TOK = 1024
OWN = 64
SEQ = 16
HD = 4
DK = 128
DV = 256
KB = 256
D = 4096
COLS = 2 * DK + 2 * DV


def softplus(x):
    return jnp.maximum(x, 0.0) + jnp.log1p(jnp.exp(-jnp.abs(x)))


def sigmoid(x):
    return 1.0 / (1.0 + jnp.exp(-x))


def silu(x):
    return x * sigmoid(x)


def place(shape):
    return lax.rem(lax.broadcasted_iota(jnp.int32, shape, 0), 4)


def back(x, j):
    return x if j == 0 else pltpu.roll(x, j, 0)


def ahead(x, j):
    return pltpu.roll(x, x.shape[0] - j, 0)


def wide(col, width):
    return jnp.broadcast_to(col, (col.shape[0], width))


def running_sum(g, at):
    c = g
    for j in (1, 2, 3):
        c = c + jnp.where(at >= j, back(g, j), 0.0)
    return c


def tail_sum(g, at):
    s = jnp.zeros_like(g)
    for j in (1, 2, 3):
        s = s + jnp.where(at + j <= 3, ahead(g, j), 0.0)
    return s


def unit(x):
    return x * lax.rsqrt(jnp.sum(x * x, -1, keepdims=True) + norm_eps)


def decays(c, at):
    out = [jnp.ones_like(c)]
    for j in (1, 2, 3):
        out.append(jnp.where(at >= j, jnp.exp(jnp.where(at >= j, c - back(c, j), 0.0)), 0.0))
    return out


def inverse_rows(k, b, w):
    low = [None]
    for j in (1, 2, 3):
        dots = jnp.sum(k * back(k, j), -1, keepdims=True)
        low.append(b * dots * w[j])
    one, two, three = low[1], low[2], low[3]
    t1 = -one
    t2 = one * back(one, 1) - two
    t3 = one * back(two, 1) + two * back(one, 2) - three - one * back(one, 1) * back(one, 2)
    return t1, t2, t3


def mixed(x, coefs):
    out = x
    for j, coef in enumerate(coefs):
        out = out + coef * back(x, j + 1)
    return out


def dot(a, b):
    return jnp.dot(a, b, preferred_element_type=F32)


def columns_of(rows):
    eye = (
        lax.broadcasted_iota(jnp.int32, (OWN, 128), 0)
        == lax.broadcasted_iota(jnp.int32, (OWN, 128), 1)
    ).astype(F32)
    return lax.dot_general(
        eye, rows, (((1,), (1,)), ((), ())), precision=HIGHEST, preferred_element_type=F32
    )


def pick(cols, at):
    lane = lax.broadcasted_iota(jnp.int32, cols.shape, 1)
    return wide(jnp.sum(jnp.where(lane == at, cols, 0.0), -1, keepdims=True), 128)


def both(x):
    return jnp.concatenate([x, x], 1)


class Sems:
    def __init__(self, send, recv):
        self.send, self.recv, self.at = send, recv, 0
        self.sent = []

    def go(self, src, dst, device):
        n = self.at
        self.at += 1
        copy = pltpu.make_async_remote_copy(
            src_ref=src,
            dst_ref=dst,
            send_sem=self.send.at[n],
            recv_sem=self.recv.at[n],
            device_id=device,
            device_id_type=MESH,
        )
        copy.start()
        self.sent.append(copy)
        return copy


N_SEM = 6 + 3 * 6 + 6 + 9 + 3 + 9 + 12 + 12 + 36
NT = (((1,), (1,)), ((), ()))


def kernel(
    hidden,
    gain,
    w_query,
    w_key,
    w_value,
    w_gate,
    w_write,
    w_decay,
    w_out,
    decay_rate,
    head_gain,
    state,
    last_keys,
    last_values,
    last_writes,
    last_decays,
    accepted,
    orecv,
    st32,
    gain_raw,
    gain32,
    rate_row,
    head_gain_row,
    old_keys,
    old_values,
    old_writes,
    old_decays,
    old_count,
    hid,
    scaled,
    wbuf,
    wsm,
    st16,
    wo,
    lhs,
    ktail,
    bv,
    tri,
    last,
    psend,
    precv,
    ssend,
    srecv,
    csend,
    proj,
    coef,
    zk,
    zq,
    gath,
    osend,
    send,
    recv,
    loc,
    o_send,
    o_recv,
):
    kv, tp = lax.axis_index("kv"), lax.axis_index("tp")
    core, y = lax.rem(tp, 2), tp // 2
    z, x = kv // 4, lax.rem(kv, 4)
    a = z + core * (x - z)
    b = x + core * (z - x)
    sa, sb = 4 - 3 * core, 1 + 3 * core

    def kv_at(a_, b_):
        return a_ * sa + b_ * sb

    def turn(i, d):
        return lax.rem(i + d + 4, 4)

    def head_cols(h, width):
        return pl.ds(pl.multiple_of(h * width, width), width)

    sems = Sems(send, recv)
    own_rows = pl.ds(pl.multiple_of(a * KB, 256), KB)

    def weight_parts(h):
        return [
            (w_query.at[:, head_cols(h, DK)], wbuf.at[0, own_rows, pl.ds(0, DK)]),
            (w_key.at[:, head_cols(h, DK)], wbuf.at[0, own_rows, pl.ds(DK, DK)]),
            (w_write, wsm.at[a, 0]),
            (w_decay, wsm.at[a, 1]),
            (w_value.at[:, head_cols(h, DV)], wbuf.at[1, own_rows, :]),
            (w_gate.at[:, head_cols(h, DV)], wbuf.at[2, own_rows, :]),
        ]

    pairs = [
        (last_keys, old_keys),
        (last_values, old_values),
        (last_writes, old_writes),
        (last_decays, old_decays),
        (accepted, old_count),
        (decay_rate, rate_row),
        (gain, gain_raw),
        (head_gain, head_gain_row),
        (hidden, hid.at[a]),
        (state, st32),
        (w_out, wo),
    ] + weight_parts(a)
    local = [pltpu.make_async_copy(src, dst, loc.at[n]) for n, (src, dst) in enumerate(pairs)]
    for copy in local:
        copy.start()

    barrier = pltpu.get_barrier_semaphore()
    for d in (1, 2, 3):
        pl.semaphore_signal(barrier, inc=1, device_id=(kv_at(turn(a, d), b), tp), device_id_type=MESH)
        pl.semaphore_signal(barrier, inc=1, device_id=(kv_at(a, turn(b, d)), tp), device_id_type=MESH)
    for e in range(1, 8):
        pl.semaphore_signal(barrier, inc=1, device_id=(kv, lax.rem(tp + e, 8)), device_id_type=MESH)
    pl.semaphore_wait(barrier, 13)

    def quarter(i):
        return pl.ds(pl.multiple_of(i * 256, 256), 256)

    hid_in = {}
    for e in (0, 2):
        for d in (1, 3, 2):
            rows = quarter(turn(y, e))
            hid_in[d, e] = sems.go(hidden.at[rows, :], hid.at[a, rows, :], (kv_at(turn(a, d), b), tp))
    w_in = {d: [] for d in (1, 2, 3)}
    for first, past in ((0, 4), (4, 5), (5, 6)):
        for d in (2, 1, 3):
            to = turn(a, d)
            for src, dst in weight_parts(to)[first:past]:
                w_in[d].append(sems.go(src, dst, (kv_at(to, b), tp)))

    for copy in local[:8]:
        copy.wait()
    gain32[...] = gain_raw[...].astype(F32)
    at = place((OWN, 128))
    which = lax.broadcasted_iota(jnp.int32, (OWN, SEQ), 0)
    seq = lax.broadcasted_iota(jnp.int32, (OWN, SEQ), 1)
    raw = jnp.zeros((OWN, 8), F32)
    for p in range(4):
        raw = raw + lax.dot_general(
            (which == 4 * seq + p).astype(F32),
            jnp.concatenate([old_writes[p], old_decays[p]], 0),
            NT,
            precision=HIGHEST,
            preferred_element_type=F32,
        )
    count = jnp.sum(jnp.where(which // 4 == seq, old_count[...].astype(F32), 0.0), -1, keepdims=True)
    taken = (place((OWN, 8)).astype(F32) < count).astype(F32)
    lane8 = lax.broadcasted_iota(jnp.int32, (OWN, 8), 1)
    rate = jnp.concatenate([rate_row[...], rate_row[...]], 1)

    def rates_and_decays(pre):
        return jnp.where(lane8 < 4, sigmoid(pre), -rate * softplus(pre))

    cols = rates_and_decays(raw) * taken

    for n in range(SEQ // 2):
        rows = slice(8 * n, 8 * n + 8)
        lhs_pair = [old_keys[2 * n + i].astype(F32) for i in (0, 1)]
        val_pair = [old_values[2 * n + i].astype(F32) for i in (0, 1)]
        for h in range(HD):
            cut = slice(h * DK, (h + 1) * DK)
            lhs[h, rows, :] = jnp.concatenate([v[:, cut] for v in lhs_pair], 0)
            cut = slice(h * DV, (h + 1) * DV)
            bv[h, rows, :] = jnp.concatenate([v[:, cut] for v in val_pair], 0)

    def old_head(h, _):
        bcol, g = pick(cols, h), pick(cols, h + 4)
        k = unit(lhs[h])
        c = running_sum(g, at)
        tail = tail_sum(g, at)
        t1, t2, t3 = inverse_rows(k, bcol, decays(c, at))
        tri[h, 0], tri[h, 1], tri[h, 2] = t1, t2, t3
        lhs[h] = bcol * k * jnp.exp(c)
        ktail[h] = k * jnp.exp(tail)
        bv[h] = both(bcol) * bv[h]
        last[h] = jnp.exp(c + tail)
        return 0

    lax.fori_loop(0, HD, old_head, 0)

    y_in = {}
    for d in (1, 3, 2):
        hid_in[d, 0].wait_recv()
        slot = turn(a, -d)
        rows = quarter(y)
        y_in[d] = [
            sems.go(hid.at[slot, rows, :], hid.at[slot, rows, :], (kv, 2 * turn(y, e) + core)) for e in (1, 3)
        ]

    local[9].wait()
    row8 = lax.broadcasted_iota(jnp.int32, (8, DV), 0)
    row8k = lax.broadcasted_iota(jnp.int32, (8, DK), 0)

    def old_pair(n, _):
        rows = pl.ds(pl.multiple_of(n * 8, 8), 8)
        for h in range(HD):
            left = lhs[h, rows, :].astype(BF16)
            s0, s1 = st32[2 * n, h], st32[2 * n + 1, h]
            zz = jnp.where(row8 < 4, dot(left, s0.astype(BF16)), dot(left, s1.astype(BF16)))
            fresh = mixed(bv[h, rows, :] - zz, [both(tri[h, j, rows, :]) for j in range(3)])
            kt = ktail[h, rows, :]
            kt2 = jnp.concatenate([jnp.where(row8k < 4, kt, 0.0), jnp.where(row8k >= 4, kt, 0.0)], 1)
            upd = lax.dot_general(
                kt2.astype(BF16), fresh.astype(BF16), (((0,), (0,)), ((), ())), preferred_element_type=F32
            )
            keep = last[h, rows, :]
            n0 = s0 * keep[0:1, 0:1] + upd[0:DK]
            n1 = s1 * keep[4:5, 0:1] + upd[DK:]
            st32[2 * n, h], st32[2 * n + 1, h] = n0, n1
            st16[2 * n, h], st16[2 * n + 1, h] = n0.astype(BF16), n1.astype(BF16)
        return 0

    lax.fori_loop(0, SEQ // 2, old_pair, 0)

    def scale_block(slot):
        row = 2 * kv_at(slot, b)
        weight = jnp.concatenate([gain32[pl.ds(row, 1), :], gain32[pl.ds(row + 1, 1), :]], 1)

        def body(n, _):
            kb, ka = n // 4, lax.rem(n, 4)
            rows = pl.ds(pl.multiple_of(kv_at(ka, kb) * OWN, OWN), OWN)
            to = pl.ds(pl.multiple_of(n * OWN, OWN), OWN)
            block = hid[slot, rows, :].astype(F32) * weight
            scaled[to, pl.ds(pl.multiple_of(slot * KB, 256), KB)] = block.astype(BF16)
            return 0

        lax.fori_loop(0, 16, body, 0)

    local[8].wait()
    scale_block(a)
    for d in (1, 3, 2):
        hid_in[d, 2].wait_recv()
        for copy in y_in[d]:
            copy.wait_recv()
        scale_block(turn(a, -d))

    p_in, c_in = {}, {}

    def send_parts(chunk, first, past):
        for copy in local[11 + first : 11 + past]:
            copy.wait()
        for d in (1, 3, 2):
            for copy in w_in[d][first:past]:
                copy.wait_recv()
        weights = wbuf[chunk]
        for d in (2, 1, 3, 0):
            to = turn(b, d)
            psend[chunk, d] = dot(scaled[quarter(to), :], weights).astype(BF16)
            if d:
                p_in[chunk, d] = sems.go(
                    psend.at[chunk, d], precv.at[chunk, d - 1], (kv_at(a, to), tp)
                )

    def send_sums(chunk):
        for d in (1, 3, 2):
            p_in[chunk, d].wait_recv()
        for d in (2, 1, 3, 0):
            to = turn(a, d)
            rows = pl.ds(pl.multiple_of(to * OWN, OWN), OWN)
            total = psend[chunk, 0, rows, :].astype(F32)
            for i in range(3):
                total = total + precv[chunk, i, rows, :].astype(F32)
            if d:
                csend[chunk, d - 1] = total.astype(BF16)
                c_in[chunk, d] = sems.go(csend.at[chunk, d - 1], proj.at[chunk, a], (kv_at(to, b), tp))
            else:
                proj[chunk, a] = total.astype(BF16)

    send_parts(0, 0, 4)
    s_in = {}
    ones = jnp.ones((8, KB), BF16)
    for d in (2, 1, 3, 0):
        to = turn(b, d)
        token = pl.ds(pl.multiple_of(kv_at(a, to) * OWN, OWN), OWN)
        mine = pl.ds(pl.multiple_of(to * 256 + a * OWN, OWN), OWN)
        write, decay = jnp.zeros((4, OWN), F32), jnp.zeros((4, OWN), F32)
        square = jnp.zeros((8, OWN), F32)
        for i in range(4):
            rows_i = scaled[mine, i * KB : (i + 1) * KB]
            write = write + lax.dot_general(wsm[i, 0], rows_i, NT, preferred_element_type=F32)
            decay = decay + lax.dot_general(wsm[i, 1], rows_i, NT, preferred_element_type=F32)
            h32 = hid[i, token, :].astype(F32)
            sq = h32 * h32
            high = sq.astype(BF16)
            low = (sq - high.astype(F32)).astype(BF16)
            square = square + lax.dot_general(ones, high, NT, preferred_element_type=F32)
            square = square + lax.dot_general(ones, low, NT, preferred_element_type=F32)
        part = jnp.concatenate([write, decay, square], 0)
        ssend[d] = jnp.concatenate([part, jnp.zeros((16, 64), F32)], 1)
        if d:
            s_in[d] = sems.go(ssend.at[d], srecv.at[d - 1], (kv_at(a, to), tp))
    send_parts(1, 4, 5)
    send_sums(0)
    send_parts(2, 5, 6)

    for d in (1, 3, 2):
        s_in[d].wait_recv()
    small = ssend[0]
    for i in range(3):
        small = small + srecv[i]
    small_cols = columns_of(small)
    inv_col = lax.rsqrt(small_cols[:, 8:9] / D + norm_eps)
    cols = rates_and_decays(small_cols[:, 0:8] * inv_col)
    send_sums(1)

    def new_keys(d):
        h = turn(a, -d)
        if d:
            c_in[0, d].wait_recv()
        bcol = pick(cols, h)
        c = running_sum(pick(cols, h + 4), at)
        w = decays(c, at)
        grow = jnp.exp(c)
        q = unit(silu(proj[0, h, :, 0:DK].astype(F32) * inv_col)) * DK ** (-0.5)
        k = unit(silu(proj[0, h, :, DK : 2 * DK].astype(F32) * inv_col))
        kl, ql = bcol * k * grow, q * grow
        for i in range(SEQ // 2):
            rows = slice(8 * i, 8 * i + 8)
            left = jnp.concatenate([kl[rows], ql[rows]], 0).astype(BF16)
            z0 = dot(left, st16[2 * i, h])
            z1 = dot(left, st16[2 * i + 1, h])
            zk[d, rows, :] = jnp.where(row8 < 4, z0[0:8], z1[0:8])
            zq[d, rows, :] = jnp.where(row8 < 4, z0[8:16], z1[8:16])
        t1, t2, t3 = inverse_rows(k, bcol, w)
        coef[d, 0], coef[d, 1], coef[d, 2] = t1, t2, t3
        for j in range(4):
            coef[d, 3 + j] = wide(jnp.sum(q * back(k, j), -1, keepdims=True), 128) * w[j]
        coef[d, 7] = bcol

    new_keys(0)
    new_keys(1)
    send_sums(2)
    new_keys(3)
    new_keys(2)

    first_in, peer_in = {}, {}
    for d in (0, 1, 3, 2):
        h = turn(a, -d)
        if d:
            c_in[1, d].wait_recv()
            c_in[2, d].wait_recv()
        v = silu(proj[1, h].astype(F32) * inv_col)
        fresh = mixed(both(coef[d, 7]) * v - zk[d], [both(coef[d, j]) for j in range(3)])
        res = zq[d]
        for j in range(4):
            res = res + both(coef[d, 3 + j]) * back(fresh, j)
        norm = res * lax.rsqrt(jnp.mean(res * res, -1, keepdims=True) + norm_eps) * head_gain_row[...]
        gath[kv, h] = (norm * silu(proj[2, h].astype(F32) * inv_col)).astype(BF16)
        block = gath.at[kv, h]
        for e in (2, 1, 3):
            first_in[e, d] = sems.go(block, block, (kv_at(turn(a, e), b), tp))
        for e in (2, 1, 3):
            peer_in[e, d] = sems.go(block, block, (kv_at(a, turn(b, e)), tp))

    on_in = {}
    for d in (0, 1, 3, 2):
        for e in (1, 3, 2):
            first_in[e, d].wait_recv()
            src = turn(a, -e)
            block = gath.at[kv_at(src, b), turn(src, -d)]
            for f in (2, 1, 3):
                on_in[e, f, d] = sems.go(block, block, (kv_at(a, turn(b, f)), tp))

    local[10].wait()
    weights = wo[...]
    outs = []

    def send_out(src, waits):
        n = len(outs)
        for copy in waits:
            copy.wait_recv()
        to, half = src // 2, lax.rem(src, 2)
        e = lax.rem(to - tp + 8, 8)
        rows = pl.ds(pl.multiple_of(half * OWN, OWN), OWN)
        total = dot(jnp.concatenate([gath[src, h] for h in range(HD)], 1), weights).astype(BF16)
        osend[n] = total
        copy = pltpu.make_async_remote_copy(
            src_ref=osend.at[n],
            dst_ref=orecv.at[e, rows, :],
            send_sem=o_send.at[n],
            recv_sem=o_recv.at[2 * e + half],
            device_id=(kv, to),
            device_id_type=MESH,
        )
        outs.append((e, copy))

        @pl.when(e != 0)
        def _():
            copy.start()

        @pl.when(e == 0)
        def _():
            orecv[0, rows, :] = total

    send_out(kv, [])
    for e in (1, 3, 2):
        send_out(kv_at(turn(a, -e), b), [])
    for e in (1, 3, 2):
        send_out(kv_at(a, turn(b, -e)), [peer_in[e, d] for d in range(4)])
    for e in (1, 3, 2):
        for f in (1, 3, 2):
            send_out(kv_at(turn(a, -e), turn(b, -f)), [on_in[e, f, d] for d in range(4)])

    for e in range(1, 8):
        for half in (0, 1):
            rows = pl.ds(half * OWN, OWN)
            pltpu.make_async_remote_copy(
                src_ref=osend.at[0],
                dst_ref=orecv.at[e, rows, :],
                send_sem=o_send.at[0],
                recv_sem=o_recv.at[2 * e + half],
                device_id=(kv, lax.rem(tp + e, 8)),
                device_id_type=MESH,
            ).wait_recv()
    for copy in sems.sent:
        copy.wait_send()
    for e, copy in outs:

        @pl.when(e != 0)
        def _():
            copy.wait_send()

    assert sems.at == N_SEM, sems.at


def mix(*args):
    hbm = pl.BlockSpec(memory_space=pl.ANY)
    vmem = pl.BlockSpec(memory_space=pltpu.VMEM)
    return pl.pallas_call(
        kernel,
        in_specs=[hbm] * 17,
        out_specs=(vmem, vmem),
        out_shape=(pltpu.VMEM((8, 128, 256), BF16), pltpu.VMEM((SEQ, HD, DK, DV), F32)),
        scratch_shapes=[
            pltpu.VMEM((32, 128), BF16),
            pltpu.VMEM((32, 128), F32),
            pltpu.VMEM((1, HD), F32),
            pltpu.VMEM((1, DV), F32),
            pltpu.VMEM((SEQ, 4, HD * DK), BF16),
            pltpu.VMEM((SEQ, 4, HD * DV), BF16),
            pltpu.VMEM((4, HD, SEQ), F32),
            pltpu.VMEM((4, HD, SEQ), F32),
            pltpu.VMEM((1, SEQ), jnp.int32),
            pltpu.VMEM((4, TOK, KB), BF16),
            pltpu.VMEM((TOK, 4 * KB), BF16),
            pltpu.VMEM((3, 4 * KB, 256), BF16),
            pltpu.VMEM((4, 2, 4, KB), BF16),
            pltpu.VMEM((SEQ, HD, DK, DV), BF16),
            pltpu.VMEM((HD * DV, 256), BF16),
            pltpu.VMEM((HD, OWN, 128), F32),
            pltpu.VMEM((HD, OWN, 128), F32),
            pltpu.VMEM((HD, OWN, DV), F32),
            pltpu.VMEM((HD, 3, OWN, 128), F32),
            pltpu.VMEM((HD, OWN, 128), F32),
            pltpu.VMEM((3, 4, 256, 256), BF16),
            pltpu.VMEM((3, 3, 256, 256), BF16),
            pltpu.VMEM((4, 16, 128), F32),
            pltpu.VMEM((3, 16, 128), F32),
            pltpu.VMEM((3, 3, OWN, 256), BF16),
            pltpu.VMEM((3, HD, OWN, 256), BF16),
            pltpu.VMEM((4, 8, OWN, 128), F32),
            pltpu.VMEM((4, OWN, DV), F32),
            pltpu.VMEM((4, OWN, DV), F32),
            pltpu.VMEM((16, HD, OWN, DV), BF16),
            pltpu.VMEM((16, OWN, 256), BF16),
            pltpu.SemaphoreType.DMA((N_SEM,)),
            pltpu.SemaphoreType.DMA((N_SEM,)),
            pltpu.SemaphoreType.DMA((17,)),
            pltpu.SemaphoreType.DMA((16,)),
            pltpu.SemaphoreType.DMA((16,)),
        ],
        compiler_params=pltpu.CompilerParams(
            collective_id=0, has_side_effects=True, vmem_limit_bytes=50 * 1024 * 1024
        ),
        name="mix",
    )(*[pltpu.with_memory_space_constraint(arg, pltpu.HBM) for arg in args])


def write_kernel(parts, states, out_ref, committed, rows, sem):
    copies = [pltpu.make_async_copy(states.at[n], committed.at[n], sem.at[n]) for n in range(SEQ)]
    for copy in copies:
        copy.start()
    total = parts[0].astype(F32)
    for i in range(1, 8):
        total = total + parts[i].astype(F32)
    rows[...] = total.astype(BF16)
    copy = pltpu.make_async_copy(rows, out_ref, sem.at[SEQ])
    copy.start()
    for other in copies:
        other.wait()
    copy.wait()


def write_out(parts, states):
    hbm = pl.BlockSpec(memory_space=pltpu.HBM)
    vmem = pl.BlockSpec(memory_space=pltpu.VMEM)
    return pl.pallas_call(
        write_kernel,
        in_specs=[vmem, vmem],
        out_specs=(hbm, hbm),
        out_shape=(jax.ShapeDtypeStruct((128, 256), BF16), jax.ShapeDtypeStruct((SEQ, HD, DK, DV), F32)),
        scratch_shapes=[pltpu.VMEM((128, 256), BF16), pltpu.SemaphoreType.DMA((SEQ + 1,))],
        compiler_params=pltpu.CompilerParams(vmem_limit_bytes=4 * 1024 * 1024),
        name="write_out",
    )(*[pltpu.with_memory_space_constraint(arg, pltpu.VMEM) for arg in (parts, states)])


def per_device(
    hidden,
    norm_gain,
    w_query,
    w_key,
    w_value,
    w_gate,
    w_write,
    w_decay,
    w_out,
    decay_rate,
    head_gain,
    carried_state,
    last_keys,
    last_values,
    last_writes,
    last_decays,
    accepted,
):
    parts, states = mix(
        hidden,
        norm_gain.reshape(32, 128),
        w_query,
        w_key,
        w_value,
        w_gate,
        w_write.T,
        w_decay.T,
        w_out,
        decay_rate.reshape(1, HD),
        head_gain.reshape(1, DV),
        carried_state,
        last_keys,
        last_values,
        jnp.transpose(last_writes, (1, 2, 0)),
        jnp.transpose(last_decays, (1, 2, 0)),
        accepted.reshape(1, SEQ),
    )
    return write_out(parts, states)


def solution(mesh):
    return jax.shard_map(
        per_device,
        mesh=mesh,
        in_specs=(
            P(None, "kv"),
            P(),
            P("kv", "tp"),
            P("kv", "tp"),
            P("kv", "tp"),
            P("kv", "tp"),
            P("kv", "tp"),
            P("kv", "tp"),
            P("tp", "kv"),
            P("tp"),
            P(),
            P("kv", "tp", None, None),
            P("kv", None, "tp"),
            P("kv", None, "tp"),
            P("kv", None, "tp"),
            P("kv", None, "tp"),
            P("kv"),
        ),
        out_specs=(P("tp", "kv"), P("kv", "tp", None, None)),
        check_vma=False,
    )
```

```python
import functools

import jax
import jax.numpy as jnp
from jax import lax
from jax.experimental import pallas as pl
from jax.experimental.pallas import tpu as pltpu
from jax.sharding import PartitionSpec as P

MESH = pl.DeviceIdType.MESH
HIGHEST = lax.Precision.HIGHEST
F32 = jnp.float32
BF16 = jnp.bfloat16
norm_eps = 1e-06

TOK = 1024
OWN = 64
SEQ = 16
HD = 4
DK = 128
DV = 256
KB = 256
D = 4096
COLS = 2 * DK + 2 * DV


def softplus(x):
    return jnp.maximum(x, 0.0) + jnp.log1p(jnp.exp(-jnp.abs(x)))


def sigmoid(x):
    return 1.0 / (1.0 + jnp.exp(-x))


def silu(x):
    return x * sigmoid(x)


def place(shape):
    return lax.rem(lax.broadcasted_iota(jnp.int32, shape, 0), 4)


def back(x, j):
    return x if j == 0 else pltpu.roll(x, j, 0)


def ahead(x, j):
    return pltpu.roll(x, x.shape[0] - j, 0)


def wide(col, width):
    return jnp.broadcast_to(col, (col.shape[0], width))


def running_sum(g, at):
    c = g
    for j in (1, 2, 3):
        c = c + jnp.where(at >= j, back(g, j), 0.0)
    return c


def tail_sum(g, at):
    s = jnp.zeros_like(g)
    for j in (1, 2, 3):
        s = s + jnp.where(at + j <= 3, ahead(g, j), 0.0)
    return s


def unit(x):
    return x * lax.rsqrt(jnp.sum(x * x, -1, keepdims=True) + norm_eps)


def decays(c, at):
    out = [jnp.ones_like(c)]
    for j in (1, 2, 3):
        out.append(jnp.where(at >= j, jnp.exp(jnp.where(at >= j, c - back(c, j), 0.0)), 0.0))
    return out


def inverse_rows(k, b, w):
    low = [None]
    for j in (1, 2, 3):
        dots = jnp.sum(k * back(k, j), -1, keepdims=True)
        low.append(b * dots * w[j])
    one, two, three = low[1], low[2], low[3]
    t1 = -one
    t2 = one * back(one, 1) - two
    t3 = one * back(two, 1) + two * back(one, 2) - three - one * back(one, 1) * back(one, 2)
    return t1, t2, t3


def mixed(x, coefs):
    out = x
    for j, coef in enumerate(coefs):
        out = out + coef * back(x, j + 1)
    return out


def dot(a, b):
    return jnp.dot(a, b, preferred_element_type=F32)


def columns_of(rows):
    eye = (
        lax.broadcasted_iota(jnp.int32, (OWN, 128), 0)
        == lax.broadcasted_iota(jnp.int32, (OWN, 128), 1)
    ).astype(F32)
    return lax.dot_general(
        eye, rows, (((1,), (1,)), ((), ())), precision=HIGHEST, preferred_element_type=F32
    )


def pick(cols, at):
    lane = lax.broadcasted_iota(jnp.int32, cols.shape, 1)
    return wide(jnp.sum(jnp.where(lane == at, cols, 0.0), -1, keepdims=True), 128)


def both(x):
    return jnp.concatenate([x, x], 1)


class Sems:
    def __init__(self, send, recv):
        self.send, self.recv, self.at = send, recv, 0
        self.sent = []

    def go(self, src, dst, device):
        n = self.at
        self.at += 1
        copy = pltpu.make_async_remote_copy(
            src_ref=src,
            dst_ref=dst,
            send_sem=self.send.at[n],
            recv_sem=self.recv.at[n],
            device_id=device,
            device_id_type=MESH,
        )
        copy.start()
        self.sent.append(copy)
        return copy


N_SEM = 6 + 3 * 6 + 6 + 9 + 3 + 9 + 2 * 19 + 30
NT = (((1,), (1,)), ((), ()))


def kernel(
    hidden,
    gain,
    w_query,
    w_key,
    w_value,
    w_gate,
    w_write,
    w_decay,
    w_out,
    decay_rate,
    head_gain,
    state,
    last_keys,
    last_values,
    last_writes,
    last_decays,
    accepted,
    orecv,
    st32,
    gain_raw,
    gain32,
    rate_row,
    head_gain_row,
    old_keys,
    old_values,
    old_writes,
    old_decays,
    old_count,
    hid,
    scaled,
    wbuf,
    wsm,
    st16,
    wo,
    lhs,
    ktail,
    bv,
    tri,
    last,
    psend,
    precv,
    ssend,
    srecv,
    csend,
    proj,
    coef,
    zk,
    zq,
    gath,
    osend,
    send,
    recv,
    loc,
    o_send,
    o_recv,
):
    kv, tp = lax.axis_index("kv"), lax.axis_index("tp")
    core, y = lax.rem(tp, 2), tp // 2
    z, x = kv // 4, lax.rem(kv, 4)
    a = z + core * (x - z)
    b = x + core * (z - x)
    sa, sb = 4 - 3 * core, 1 + 3 * core

    def kv_at(a_, b_):
        return a_ * sa + b_ * sb

    def turn(i, d):
        return lax.rem(i + d + 4, 4)

    def head_cols(h, width):
        return pl.ds(pl.multiple_of(h * width, width), width)

    sems = Sems(send, recv)
    own_rows = pl.ds(pl.multiple_of(a * KB, 256), KB)

    def weight_parts(h):
        return [
            (w_query.at[:, head_cols(h, DK)], wbuf.at[0, own_rows, pl.ds(0, DK)]),
            (w_key.at[:, head_cols(h, DK)], wbuf.at[0, own_rows, pl.ds(DK, DK)]),
            (w_write, wsm.at[a, 0]),
            (w_decay, wsm.at[a, 1]),
            (w_value.at[:, head_cols(h, DV)], wbuf.at[1, own_rows, :]),
            (w_gate.at[:, head_cols(h, DV)], wbuf.at[2, own_rows, :]),
        ]

    pairs = [
        (last_keys, old_keys),
        (last_values, old_values),
        (last_writes, old_writes),
        (last_decays, old_decays),
        (accepted, old_count),
        (decay_rate, rate_row),
        (gain, gain_raw),
        (head_gain, head_gain_row),
        (hidden, hid.at[a]),
        (state, st32),
        (w_out, wo),
    ] + weight_parts(a)
    local = [pltpu.make_async_copy(src, dst, loc.at[n]) for n, (src, dst) in enumerate(pairs)]
    for copy in local:
        copy.start()

    barrier = pltpu.get_barrier_semaphore()
    for d in (1, 2, 3):
        pl.semaphore_signal(barrier, inc=1, device_id=(kv_at(turn(a, d), b), tp), device_id_type=MESH)
        pl.semaphore_signal(barrier, inc=1, device_id=(kv_at(a, turn(b, d)), tp), device_id_type=MESH)
    for e in range(1, 8):
        pl.semaphore_signal(barrier, inc=1, device_id=(kv, lax.rem(tp + e, 8)), device_id_type=MESH)
    pl.semaphore_wait(barrier, 13)

    def quarter(i):
        return pl.ds(pl.multiple_of(i * 256, 256), 256)

    hid_in = {}
    for e in (0, 2):
        for d in (1, 3, 2):
            rows = quarter(turn(y, e))
            hid_in[d, e] = sems.go(hidden.at[rows, :], hid.at[a, rows, :], (kv_at(turn(a, d), b), tp))
    w_in = {d: [] for d in (1, 2, 3)}
    for first, past in ((0, 4), (4, 5), (5, 6)):
        for d in (2, 1, 3):
            to = turn(a, d)
            for src, dst in weight_parts(to)[first:past]:
                w_in[d].append(sems.go(src, dst, (kv_at(to, b), tp)))

    for copy in local[:8]:
        copy.wait()
    gain32[...] = gain_raw[...].astype(F32)
    at = place((OWN, 128))
    which = lax.broadcasted_iota(jnp.int32, (OWN, SEQ), 0)
    seq = lax.broadcasted_iota(jnp.int32, (OWN, SEQ), 1)
    raw = jnp.zeros((OWN, 8), F32)
    for p in range(4):
        raw = raw + lax.dot_general(
            (which == 4 * seq + p).astype(F32),
            jnp.concatenate([old_writes[p], old_decays[p]], 0),
            NT,
            precision=HIGHEST,
            preferred_element_type=F32,
        )
    count = jnp.sum(jnp.where(which // 4 == seq, old_count[...].astype(F32), 0.0), -1, keepdims=True)
    taken = (place((OWN, 8)).astype(F32) < count).astype(F32)
    lane8 = lax.broadcasted_iota(jnp.int32, (OWN, 8), 1)
    rate = jnp.concatenate([rate_row[...], rate_row[...]], 1)

    def rates_and_decays(pre):
        return jnp.where(lane8 < 4, sigmoid(pre), -rate * softplus(pre))

    cols = rates_and_decays(raw) * taken

    for n in range(SEQ // 2):
        rows = slice(8 * n, 8 * n + 8)
        lhs_pair = [old_keys[2 * n + i].astype(F32) for i in (0, 1)]
        val_pair = [old_values[2 * n + i].astype(F32) for i in (0, 1)]
        for h in range(HD):
            cut = slice(h * DK, (h + 1) * DK)
            lhs[h, rows, :] = jnp.concatenate([v[:, cut] for v in lhs_pair], 0)
            cut = slice(h * DV, (h + 1) * DV)
            bv[h, rows, :] = jnp.concatenate([v[:, cut] for v in val_pair], 0)

    def old_head(h, _):
        bcol, g = pick(cols, h), pick(cols, h + 4)
        k = unit(lhs[h])
        c = running_sum(g, at)
        tail = tail_sum(g, at)
        t1, t2, t3 = inverse_rows(k, bcol, decays(c, at))
        tri[h, 0], tri[h, 1], tri[h, 2] = t1, t2, t3
        lhs[h] = bcol * k * jnp.exp(c)
        ktail[h] = k * jnp.exp(tail)
        bv[h] = both(bcol) * bv[h]
        last[h] = jnp.exp(c + tail)
        return 0

    lax.fori_loop(0, HD, old_head, 0)

    y_in = {}
    for d in (1, 3, 2):
        hid_in[d, 0].wait_recv()
        slot = turn(a, -d)
        rows = quarter(y)
        y_in[d] = [
            sems.go(hid.at[slot, rows, :], hid.at[slot, rows, :], (kv, 2 * turn(y, e) + core)) for e in (1, 3)
        ]

    local[9].wait()
    row8 = lax.broadcasted_iota(jnp.int32, (8, DV), 0)
    row8k = lax.broadcasted_iota(jnp.int32, (8, DK), 0)

    def old_pair(n, _):
        rows = pl.ds(pl.multiple_of(n * 8, 8), 8)
        for h in range(HD):
            left = lhs[h, rows, :].astype(BF16)
            s0, s1 = st32[2 * n, h], st32[2 * n + 1, h]
            zz = jnp.where(row8 < 4, dot(left, s0.astype(BF16)), dot(left, s1.astype(BF16)))
            fresh = mixed(bv[h, rows, :] - zz, [both(tri[h, j, rows, :]) for j in range(3)])
            kt = ktail[h, rows, :]
            kt2 = jnp.concatenate([jnp.where(row8k < 4, kt, 0.0), jnp.where(row8k >= 4, kt, 0.0)], 1)
            upd = lax.dot_general(
                kt2.astype(BF16), fresh.astype(BF16), (((0,), (0,)), ((), ())), preferred_element_type=F32
            )
            keep = last[h, rows, :]
            n0 = s0 * keep[0:1, 0:1] + upd[0:DK]
            n1 = s1 * keep[4:5, 0:1] + upd[DK:]
            st32[2 * n, h], st32[2 * n + 1, h] = n0, n1
            st16[2 * n, h], st16[2 * n + 1, h] = n0.astype(BF16), n1.astype(BF16)
        return 0

    lax.fori_loop(0, SEQ // 2, old_pair, 0)

    def scale_block(slot):
        row = 2 * kv_at(slot, b)
        weight = jnp.concatenate([gain32[pl.ds(row, 1), :], gain32[pl.ds(row + 1, 1), :]], 1)

        def body(n, _):
            kb, ka = n // 4, lax.rem(n, 4)
            rows = pl.ds(pl.multiple_of(kv_at(ka, kb) * OWN, OWN), OWN)
            to = pl.ds(pl.multiple_of(n * OWN, OWN), OWN)
            block = hid[slot, rows, :].astype(F32) * weight
            scaled[to, pl.ds(pl.multiple_of(slot * KB, 256), KB)] = block.astype(BF16)
            return 0

        lax.fori_loop(0, 16, body, 0)

    local[8].wait()
    scale_block(a)
    for d in (1, 3, 2):
        hid_in[d, 2].wait_recv()
        for copy in y_in[d]:
            copy.wait_recv()
        scale_block(turn(a, -d))

    p_in, c_in = {}, {}

    def send_parts(chunk, first, past):
        for copy in local[11 + first : 11 + past]:
            copy.wait()
        for d in (1, 3, 2):
            for copy in w_in[d][first:past]:
                copy.wait_recv()
        weights = wbuf[chunk]
        for d in (2, 1, 3, 0):
            to = turn(b, d)
            psend[chunk, d] = dot(scaled[quarter(to), :], weights).astype(BF16)
            if d:
                p_in[chunk, d] = sems.go(
                    psend.at[chunk, d], precv.at[chunk, d - 1], (kv_at(a, to), tp)
                )

    def send_sums(chunk):
        for d in (1, 3, 2):
            p_in[chunk, d].wait_recv()
        for d in (2, 1, 3, 0):
            to = turn(a, d)
            rows = pl.ds(pl.multiple_of(to * OWN, OWN), OWN)
            total = psend[chunk, 0, rows, :].astype(F32)
            for i in range(3):
                total = total + precv[chunk, i, rows, :].astype(F32)
            if d:
                csend[chunk, d - 1] = total.astype(BF16)
                c_in[chunk, d] = sems.go(csend.at[chunk, d - 1], proj.at[chunk, a], (kv_at(to, b), tp))
            else:
                proj[chunk, a] = total.astype(BF16)

    send_parts(0, 0, 4)
    s_in = {}
    ones = jnp.ones((8, KB), BF16)
    for d in (2, 1, 3, 0):
        to = turn(b, d)
        token = pl.ds(pl.multiple_of(kv_at(a, to) * OWN, OWN), OWN)
        mine = pl.ds(pl.multiple_of(to * 256 + a * OWN, OWN), OWN)
        write, decay = jnp.zeros((4, OWN), F32), jnp.zeros((4, OWN), F32)
        square = jnp.zeros((8, OWN), F32)
        for i in range(4):
            rows_i = scaled[mine, i * KB : (i + 1) * KB]
            write = write + lax.dot_general(wsm[i, 0], rows_i, NT, preferred_element_type=F32)
            decay = decay + lax.dot_general(wsm[i, 1], rows_i, NT, preferred_element_type=F32)
            h32 = hid[i, token, :].astype(F32)
            sq = h32 * h32
            high = sq.astype(BF16)
            low = (sq - high.astype(F32)).astype(BF16)
            square = square + lax.dot_general(ones, high, NT, preferred_element_type=F32)
            square = square + lax.dot_general(ones, low, NT, preferred_element_type=F32)
        part = jnp.concatenate([write, decay, square], 0)
        ssend[d] = jnp.concatenate([part, jnp.zeros((16, 64), F32)], 1)
        if d:
            s_in[d] = sems.go(ssend.at[d], srecv.at[d - 1], (kv_at(a, to), tp))
    send_parts(1, 4, 5)
    send_sums(0)
    send_parts(2, 5, 6)

    for d in (1, 3, 2):
        s_in[d].wait_recv()
    small = ssend[0]
    for i in range(3):
        small = small + srecv[i]
    small_cols = columns_of(small)
    inv_col = lax.rsqrt(small_cols[:, 8:9] / D + norm_eps)
    cols = rates_and_decays(small_cols[:, 0:8] * inv_col)
    send_sums(1)

    def new_keys(d):
        h = turn(a, -d)
        if d:
            c_in[0, d].wait_recv()
        bcol = pick(cols, h)
        c = running_sum(pick(cols, h + 4), at)
        w = decays(c, at)
        grow = jnp.exp(c)
        q = unit(silu(proj[0, h, :, 0:DK].astype(F32) * inv_col)) * DK ** (-0.5)
        k = unit(silu(proj[0, h, :, DK : 2 * DK].astype(F32) * inv_col))
        kl, ql = bcol * k * grow, q * grow
        for i in range(SEQ // 2):
            rows = slice(8 * i, 8 * i + 8)
            left = jnp.concatenate([kl[rows], ql[rows]], 0).astype(BF16)
            z0 = dot(left, st16[2 * i, h])
            z1 = dot(left, st16[2 * i + 1, h])
            zk[d, rows, :] = jnp.where(row8 < 4, z0[0:8], z1[0:8])
            zq[d, rows, :] = jnp.where(row8 < 4, z0[8:16], z1[8:16])
        t1, t2, t3 = inverse_rows(k, bcol, w)
        coef[d, 0], coef[d, 1], coef[d, 2] = t1, t2, t3
        for j in range(4):
            coef[d, 3 + j] = wide(jnp.sum(q * back(k, j), -1, keepdims=True), 128) * w[j]
        coef[d, 7] = bcol

    new_keys(0)
    new_keys(1)
    send_sums(2)
    new_keys(3)
    new_keys(2)

    def gated(ea, fb, d):
        src = turn(a, -ea)
        return gath.at[kv_at(src, turn(b, -fb)), turn(src, -d)]

    def along_a(s):
        return (kv_at(turn(a, s), b), tp)

    def along_b(s):
        return (kv_at(a, turn(b, s)), tp)

    def half_of(block, s):
        return block.at[pl.ds(OWN // 2 * (s // 2), OWN // 2), :]

    b_near, b_far = {}, {}
    first_in, peer_in, on_in = {}, {}, {}

    def new_rows(d):
        h = turn(a, -d)
        if d:
            c_in[1, d].wait_recv()
            c_in[2, d].wait_recv()
        v = silu(proj[1, h].astype(F32) * inv_col)
        fresh = mixed(both(coef[d, 7]) * v - zk[d], [both(coef[d, j]) for j in range(3)])
        res = zq[d]
        for j in range(4):
            res = res + both(coef[d, 3 + j]) * back(fresh, j)
        norm = res * lax.rsqrt(jnp.mean(res * res, -1, keepdims=True) + norm_eps) * head_gain_row[...]
        gath[kv, h] = (norm * silu(proj[2, h].astype(F32) * inv_col)).astype(BF16)

    def b_first(ea, d):
        block = gated(ea, 0, d)
        for s in (1, 3):
            b_near[ea, s, d] = sems.go(block, block, along_b(s))

    def b_relay(ea, d):
        for s in (1, 3):
            b_near[ea, s, d].wait_recv()
            block = half_of(gated(ea, s, d), s)
            b_far[ea, s, d] = sems.go(block, block, along_b(s))

    def start(d, direct=False):
        new_rows(d)
        block = gated(0, 0, d)
        for e in (2, 1, 3):
            first_in[e, d] = sems.go(block, block, along_a(e))
        if direct:
            for e in (2, 1, 3):
                peer_in[e, d] = sems.go(block, block, along_b(e))
        else:
            b_first(0, d)

    def hand_on(d, direct=False):
        for e in (1, 3, 2):
            first_in[e, d].wait_recv()
            if direct:
                block = gated(e, 0, d)
                for f in (2, 1, 3):
                    on_in[e, f, d] = sems.go(block, block, along_b(f))
            else:
                b_first(e, d)

    start(0)
    start(1)
    start(3, True)
    start(2, True)
    for d in (0, 1):
        b_relay(0, d)
        hand_on(d)
    hand_on(3, True)
    hand_on(2, True)
    for d in (0, 1):
        for e in (1, 3, 2):
            b_relay(e, d)

    def arrived(ea, fb):
        waits = []
        if fb == 2:
            waits += [b_far[ea, s, d] for d in (0, 1) for s in (1, 3)]
        if fb and ea:
            waits += [on_in[ea, fb, 3], on_in[ea, fb, 2]]
        elif fb:
            waits += [peer_in[fb, 3], peer_in[fb, 2]]
        return waits

    local[10].wait()
    weights = wo[...]
    outs = []

    def send_out(src, waits):
        n = len(outs)
        for copy in waits:
            copy.wait_recv()
        to, half = src // 2, lax.rem(src, 2)
        e = lax.rem(to - tp + 8, 8)
        rows = pl.ds(pl.multiple_of(half * OWN, OWN), OWN)
        total = dot(jnp.concatenate([gath[src, h] for h in range(HD)], 1), weights).astype(BF16)
        osend[n] = total
        copy = pltpu.make_async_remote_copy(
            src_ref=osend.at[n],
            dst_ref=orecv.at[e, rows, :],
            send_sem=o_send.at[n],
            recv_sem=o_recv.at[2 * e + half],
            device_id=(kv, to),
            device_id_type=MESH,
        )
        outs.append((e, copy))

        @pl.when(e != 0)
        def _():
            copy.start()

        @pl.when(e == 0)
        def _():
            orecv[0, rows, :] = total

    for ea, fb in ((0, 0), (1, 0), (3, 0), (2, 0), (0, 1), (0, 3), (0, 2)):
        send_out(kv_at(turn(a, -ea), turn(b, -fb)), arrived(ea, fb))
    for fb in (1, 3, 2):
        for ea in (1, 3, 2):
            send_out(kv_at(turn(a, -ea), turn(b, -fb)), arrived(ea, fb))

    for e in range(1, 8):
        for half in (0, 1):
            rows = pl.ds(half * OWN, OWN)
            pltpu.make_async_remote_copy(
                src_ref=osend.at[0],
                dst_ref=orecv.at[e, rows, :],
                send_sem=o_send.at[0],
                recv_sem=o_recv.at[2 * e + half],
                device_id=(kv, lax.rem(tp + e, 8)),
                device_id_type=MESH,
            ).wait_recv()
    for copy in sems.sent:
        copy.wait_send()
    for e, copy in outs:

        @pl.when(e != 0)
        def _():
            copy.wait_send()

    assert sems.at == N_SEM, sems.at


def mix(*args):
    hbm = pl.BlockSpec(memory_space=pl.ANY)
    vmem = pl.BlockSpec(memory_space=pltpu.VMEM)
    return pl.pallas_call(
        kernel,
        in_specs=[hbm] * 17,
        out_specs=(vmem, vmem),
        out_shape=(pltpu.VMEM((8, 128, 256), BF16), pltpu.VMEM((SEQ, HD, DK, DV), F32)),
        scratch_shapes=[
            pltpu.VMEM((32, 128), BF16),
            pltpu.VMEM((32, 128), F32),
            pltpu.VMEM((1, HD), F32),
            pltpu.VMEM((1, DV), F32),
            pltpu.VMEM((SEQ, 4, HD * DK), BF16),
            pltpu.VMEM((SEQ, 4, HD * DV), BF16),
            pltpu.VMEM((4, HD, SEQ), F32),
            pltpu.VMEM((4, HD, SEQ), F32),
            pltpu.VMEM((1, SEQ), jnp.int32),
            pltpu.VMEM((4, TOK, KB), BF16),
            pltpu.VMEM((TOK, 4 * KB), BF16),
            pltpu.VMEM((3, 4 * KB, 256), BF16),
            pltpu.VMEM((4, 2, 4, KB), BF16),
            pltpu.VMEM((SEQ, HD, DK, DV), BF16),
            pltpu.VMEM((HD * DV, 256), BF16),
            pltpu.VMEM((HD, OWN, 128), F32),
            pltpu.VMEM((HD, OWN, 128), F32),
            pltpu.VMEM((HD, OWN, DV), F32),
            pltpu.VMEM((HD, 3, OWN, 128), F32),
            pltpu.VMEM((HD, OWN, 128), F32),
            pltpu.VMEM((3, 4, 256, 256), BF16),
            pltpu.VMEM((3, 3, 256, 256), BF16),
            pltpu.VMEM((4, 16, 128), F32),
            pltpu.VMEM((3, 16, 128), F32),
            pltpu.VMEM((3, 3, OWN, 256), BF16),
            pltpu.VMEM((3, HD, OWN, 256), BF16),
            pltpu.VMEM((4, 8, OWN, 128), F32),
            pltpu.VMEM((4, OWN, DV), F32),
            pltpu.VMEM((4, OWN, DV), F32),
            pltpu.VMEM((16, HD, OWN, DV), BF16),
            pltpu.VMEM((16, OWN, 256), BF16),
            pltpu.SemaphoreType.DMA((N_SEM,)),
            pltpu.SemaphoreType.DMA((N_SEM,)),
            pltpu.SemaphoreType.DMA((17,)),
            pltpu.SemaphoreType.DMA((16,)),
            pltpu.SemaphoreType.DMA((16,)),
        ],
        compiler_params=pltpu.CompilerParams(
            collective_id=0, has_side_effects=True, vmem_limit_bytes=50 * 1024 * 1024
        ),
        name="mix",
    )(*[pltpu.with_memory_space_constraint(arg, pltpu.HBM) for arg in args])


def write_kernel(parts, states, out_ref, committed, rows, sem):
    copies = [pltpu.make_async_copy(states.at[n], committed.at[n], sem.at[n]) for n in range(SEQ)]
    for copy in copies:
        copy.start()
    total = parts[0].astype(F32)
    for i in range(1, 8):
        total = total + parts[i].astype(F32)
    rows[...] = total.astype(BF16)
    copy = pltpu.make_async_copy(rows, out_ref, sem.at[SEQ])
    copy.start()
    for other in copies:
        other.wait()
    copy.wait()


def write_out(parts, states):
    hbm = pl.BlockSpec(memory_space=pltpu.HBM)
    vmem = pl.BlockSpec(memory_space=pltpu.VMEM)
    return pl.pallas_call(
        write_kernel,
        in_specs=[vmem, vmem],
        out_specs=(hbm, hbm),
        out_shape=(jax.ShapeDtypeStruct((128, 256), BF16), jax.ShapeDtypeStruct((SEQ, HD, DK, DV), F32)),
        scratch_shapes=[pltpu.VMEM((128, 256), BF16), pltpu.SemaphoreType.DMA((SEQ + 1,))],
        compiler_params=pltpu.CompilerParams(vmem_limit_bytes=4 * 1024 * 1024),
        name="write_out",
    )(*[pltpu.with_memory_space_constraint(arg, pltpu.VMEM) for arg in (parts, states)])


def per_device(
    hidden,
    norm_gain,
    w_query,
    w_key,
    w_value,
    w_gate,
    w_write,
    w_decay,
    w_out,
    decay_rate,
    head_gain,
    carried_state,
    last_keys,
    last_values,
    last_writes,
    last_decays,
    accepted,
):
    parts, states = mix(
        hidden,
        norm_gain.reshape(32, 128),
        w_query,
        w_key,
        w_value,
        w_gate,
        w_write.T,
        w_decay.T,
        w_out,
        decay_rate.reshape(1, HD),
        head_gain.reshape(1, DV),
        carried_state,
        last_keys,
        last_values,
        jnp.transpose(last_writes, (1, 2, 0)),
        jnp.transpose(last_decays, (1, 2, 0)),
        accepted.reshape(1, SEQ),
    )
    return write_out(parts, states)


def solution(mesh):
    return jax.shard_map(
        per_device,
        mesh=mesh,
        in_specs=(
            P(None, "kv"),
            P(),
            P("kv", "tp"),
            P("kv", "tp"),
            P("kv", "tp"),
            P("kv", "tp"),
            P("kv", "tp"),
            P("kv", "tp"),
            P("tp", "kv"),
            P("tp"),
            P(),
            P("kv", "tp", None, None),
            P("kv", None, "tp"),
            P("kv", None, "tp"),
            P("kv", None, "tp"),
            P("kv", None, "tp"),
            P("kv"),
        ),
        out_specs=(P("tp", "kv"), P("kv", "tp", None, None)),
        check_vma=False,
    )
```

```python
import functools

import jax
import jax.numpy as jnp
from jax import lax
from jax.experimental import pallas as pl
from jax.experimental.pallas import tpu as pltpu
from jax.sharding import PartitionSpec as P

MESH = pl.DeviceIdType.MESH
HIGHEST = lax.Precision.HIGHEST
F32 = jnp.float32
BF16 = jnp.bfloat16
norm_eps = 1e-06

TOK = 1024
OWN = 64
SEQ = 16
HD = 4
DK = 128
DV = 256
KB = 256
D = 4096
COLS = 2 * DK + 2 * DV


def softplus(x):
    return jnp.maximum(x, 0.0) + jnp.log1p(jnp.exp(-jnp.abs(x)))


def sigmoid(x):
    return 1.0 / (1.0 + jnp.exp(-x))


def silu(x):
    return x * sigmoid(x)


def place(shape):
    return lax.rem(lax.broadcasted_iota(jnp.int32, shape, 0), 4)


def back(x, j):
    return x if j == 0 else pltpu.roll(x, j, 0)


def ahead(x, j):
    return pltpu.roll(x, x.shape[0] - j, 0)


def wide(col, width):
    return jnp.broadcast_to(col, (col.shape[0], width))


def running_sum(g, at):
    c = g
    for j in (1, 2, 3):
        c = c + jnp.where(at >= j, back(g, j), 0.0)
    return c


def tail_sum(g, at):
    s = jnp.zeros_like(g)
    for j in (1, 2, 3):
        s = s + jnp.where(at + j <= 3, ahead(g, j), 0.0)
    return s


def unit(x):
    return x * lax.rsqrt(jnp.sum(x * x, -1, keepdims=True) + norm_eps)


def decays(c, at):
    out = [jnp.ones_like(c)]
    for j in (1, 2, 3):
        out.append(jnp.where(at >= j, jnp.exp(jnp.where(at >= j, c - back(c, j), 0.0)), 0.0))
    return out


def inverse_rows(k, b, w):
    low = [None]
    for j in (1, 2, 3):
        dots = jnp.sum(k * back(k, j), -1, keepdims=True)
        low.append(b * dots * w[j])
    one, two, three = low[1], low[2], low[3]
    t1 = -one
    t2 = one * back(one, 1) - two
    t3 = one * back(two, 1) + two * back(one, 2) - three - one * back(one, 1) * back(one, 2)
    return t1, t2, t3


def mixed(x, coefs):
    out = x
    for j, coef in enumerate(coefs):
        out = out + coef * back(x, j + 1)
    return out


def dot(a, b):
    return jnp.dot(a, b, preferred_element_type=F32)


def columns_of(rows):
    eye = (
        lax.broadcasted_iota(jnp.int32, (OWN, 128), 0)
        == lax.broadcasted_iota(jnp.int32, (OWN, 128), 1)
    ).astype(F32)
    return lax.dot_general(
        eye, rows, (((1,), (1,)), ((), ())), precision=HIGHEST, preferred_element_type=F32
    )


def pick(cols, at):
    lane = lax.broadcasted_iota(jnp.int32, cols.shape, 1)
    return wide(jnp.sum(jnp.where(lane == at, cols, 0.0), -1, keepdims=True), 128)


def both(x):
    return jnp.concatenate([x, x], 1)


class Sems:
    def __init__(self, send, recv):
        self.send, self.recv, self.at = send, recv, 0
        self.sent = []

    def go(self, src, dst, device):
        n = self.at
        self.at += 1
        copy = pltpu.make_async_remote_copy(
            src_ref=src,
            dst_ref=dst,
            send_sem=self.send.at[n],
            recv_sem=self.recv.at[n],
            device_id=device,
            device_id_type=MESH,
        )
        copy.start()
        self.sent.append(copy)
        return copy


N_SEM = 12 + 3 * 6 + 12 + 9 + 3 + 9 + 2 * 19 + 30
NT = (((1,), (1,)), ((), ()))


def kernel(
    hidden,
    gain,
    w_query,
    w_key,
    w_value,
    w_gate,
    w_write,
    w_decay,
    w_out,
    decay_rate,
    head_gain,
    state,
    last_keys,
    last_values,
    last_writes,
    last_decays,
    accepted,
    orecv,
    st32,
    gain_raw,
    gain32,
    rate_row,
    head_gain_row,
    old_keys,
    old_values,
    old_writes,
    old_decays,
    old_count,
    hid,
    scaled,
    wbuf,
    wsm,
    st16,
    wo,
    lhs,
    ktail,
    bv,
    tri,
    last,
    psend,
    precv,
    ssend,
    srecv,
    csend,
    proj,
    coef,
    zk,
    zq,
    gath,
    osend,
    send,
    recv,
    loc,
    o_send,
    o_recv,
):
    kv, tp = lax.axis_index("kv"), lax.axis_index("tp")
    core, y = lax.rem(tp, 2), tp // 2
    z, x = kv // 4, lax.rem(kv, 4)
    a = z + core * (x - z)
    b = x + core * (z - x)
    sa, sb = 4 - 3 * core, 1 + 3 * core

    def kv_at(a_, b_):
        return a_ * sa + b_ * sb

    def turn(i, d):
        return lax.rem(i + d + 4, 4)

    def head_cols(h, width):
        return pl.ds(pl.multiple_of(h * width, width), width)

    sems = Sems(send, recv)
    own_rows = pl.ds(pl.multiple_of(a * KB, 256), KB)

    def weight_parts(h):
        return [
            (w_query.at[:, head_cols(h, DK)], wbuf.at[0, own_rows, pl.ds(0, DK)]),
            (w_key.at[:, head_cols(h, DK)], wbuf.at[0, own_rows, pl.ds(DK, DK)]),
            (w_write, wsm.at[a, 0]),
            (w_decay, wsm.at[a, 1]),
            (w_value.at[:, head_cols(h, DV)], wbuf.at[1, own_rows, :]),
            (w_gate.at[:, head_cols(h, DV)], wbuf.at[2, own_rows, :]),
        ]

    pairs = [
        (last_keys, old_keys),
        (last_values, old_values),
        (last_writes, old_writes),
        (last_decays, old_decays),
        (accepted, old_count),
        (decay_rate, rate_row),
        (gain, gain_raw),
        (head_gain, head_gain_row),
        (hidden, hid.at[a]),
        (state, st32),
        (w_out, wo),
    ] + weight_parts(a)
    local = [pltpu.make_async_copy(src, dst, loc.at[n]) for n, (src, dst) in enumerate(pairs)]
    for copy in local:
        copy.start()

    barrier = pltpu.get_barrier_semaphore()
    for d in (1, 2, 3):
        pl.semaphore_signal(barrier, inc=1, device_id=(kv_at(turn(a, d), b), tp), device_id_type=MESH)
        pl.semaphore_signal(barrier, inc=1, device_id=(kv_at(a, turn(b, d)), tp), device_id_type=MESH)
    for e in range(1, 8):
        pl.semaphore_signal(barrier, inc=1, device_id=(kv, lax.rem(tp + e, 8)), device_id_type=MESH)
    pl.semaphore_wait(barrier, 13)

    def quarter(i):
        return pl.ds(pl.multiple_of(i * 256, 256), 256)

    hid_in = {}

    def rows_of(i, part):
        return pl.ds(pl.multiple_of(i * 256 + part * 128, 128), 128)

    for e in (0, 2):
        for part in (0, 1):
            for d in (1, 3, 2):
                rows = rows_of(turn(y, e), part)
                hid_in[d, e, part] = sems.go(
                    hidden.at[rows, :], hid.at[a, rows, :], (kv_at(turn(a, d), b), tp)
                )
    w_in = {d: [] for d in (1, 2, 3)}
    for first, past in ((0, 4), (4, 5), (5, 6)):
        for d in (2, 1, 3):
            to = turn(a, d)
            for src, dst in weight_parts(to)[first:past]:
                w_in[d].append(sems.go(src, dst, (kv_at(to, b), tp)))

    for copy in local[:8]:
        copy.wait()
    gain32[...] = gain_raw[...].astype(F32)
    at = place((OWN, 128))
    which = lax.broadcasted_iota(jnp.int32, (OWN, SEQ), 0)
    seq = lax.broadcasted_iota(jnp.int32, (OWN, SEQ), 1)
    raw = jnp.zeros((OWN, 8), F32)
    for p in range(4):
        raw = raw + lax.dot_general(
            (which == 4 * seq + p).astype(F32),
            jnp.concatenate([old_writes[p], old_decays[p]], 0),
            NT,
            precision=HIGHEST,
            preferred_element_type=F32,
        )
    count = jnp.sum(jnp.where(which // 4 == seq, old_count[...].astype(F32), 0.0), -1, keepdims=True)
    taken = (place((OWN, 8)).astype(F32) < count).astype(F32)
    lane8 = lax.broadcasted_iota(jnp.int32, (OWN, 8), 1)
    rate = jnp.concatenate([rate_row[...], rate_row[...]], 1)

    def rates_and_decays(pre):
        return jnp.where(lane8 < 4, sigmoid(pre), -rate * softplus(pre))

    cols = rates_and_decays(raw) * taken

    for n in range(SEQ // 2):
        rows = slice(8 * n, 8 * n + 8)
        lhs_pair = [old_keys[2 * n + i].astype(F32) for i in (0, 1)]
        val_pair = [old_values[2 * n + i].astype(F32) for i in (0, 1)]
        for h in range(HD):
            cut = slice(h * DK, (h + 1) * DK)
            lhs[h, rows, :] = jnp.concatenate([v[:, cut] for v in lhs_pair], 0)
            cut = slice(h * DV, (h + 1) * DV)
            bv[h, rows, :] = jnp.concatenate([v[:, cut] for v in val_pair], 0)

    y_in = {1: [], 2: [], 3: []}
    for part in (0, 1):
        for d in (1, 3, 2):
            hid_in[d, 0, part].wait_recv()
            block = hid.at[turn(a, -d), rows_of(y, part), :]
            for e in (1, 3):
                y_in[d].append(sems.go(block, block, (kv, 2 * turn(y, e) + core)))

    def old_head(h, _):
        bcol, g = pick(cols, h), pick(cols, h + 4)
        k = unit(lhs[h])
        c = running_sum(g, at)
        tail = tail_sum(g, at)
        t1, t2, t3 = inverse_rows(k, bcol, decays(c, at))
        tri[h, 0], tri[h, 1], tri[h, 2] = t1, t2, t3
        lhs[h] = bcol * k * jnp.exp(c)
        ktail[h] = k * jnp.exp(tail)
        bv[h] = both(bcol) * bv[h]
        last[h] = jnp.exp(c + tail)
        return 0

    lax.fori_loop(0, HD, old_head, 0)

    local[9].wait()
    row8 = lax.broadcasted_iota(jnp.int32, (8, DV), 0)
    row8k = lax.broadcasted_iota(jnp.int32, (8, DK), 0)

    def old_pair(n, _):
        rows = pl.ds(pl.multiple_of(n * 8, 8), 8)
        for h in range(HD):
            left = lhs[h, rows, :].astype(BF16)
            s0, s1 = st32[2 * n, h], st32[2 * n + 1, h]
            zz = jnp.where(row8 < 4, dot(left, s0.astype(BF16)), dot(left, s1.astype(BF16)))
            fresh = mixed(bv[h, rows, :] - zz, [both(tri[h, j, rows, :]) for j in range(3)])
            kt = ktail[h, rows, :]
            kt2 = jnp.concatenate([jnp.where(row8k < 4, kt, 0.0), jnp.where(row8k >= 4, kt, 0.0)], 1)
            upd = lax.dot_general(
                kt2.astype(BF16), fresh.astype(BF16), (((0,), (0,)), ((), ())), preferred_element_type=F32
            )
            keep = last[h, rows, :]
            n0 = s0 * keep[0:1, 0:1] + upd[0:DK]
            n1 = s1 * keep[4:5, 0:1] + upd[DK:]
            st32[2 * n, h], st32[2 * n + 1, h] = n0, n1
            st16[2 * n, h], st16[2 * n + 1, h] = n0.astype(BF16), n1.astype(BF16)
        return 0

    lax.fori_loop(0, SEQ // 2, old_pair, 0)

    def scale_block(slot):
        row = 2 * kv_at(slot, b)
        weight = jnp.concatenate([gain32[pl.ds(row, 1), :], gain32[pl.ds(row + 1, 1), :]], 1)

        def body(n, _):
            kb, ka = n // 4, lax.rem(n, 4)
            rows = pl.ds(pl.multiple_of(kv_at(ka, kb) * OWN, OWN), OWN)
            to = pl.ds(pl.multiple_of(n * OWN, OWN), OWN)
            block = hid[slot, rows, :].astype(F32) * weight
            scaled[to, pl.ds(pl.multiple_of(slot * KB, 256), KB)] = block.astype(BF16)
            return 0

        lax.fori_loop(0, 16, body, 0)

    local[8].wait()
    scale_block(a)
    for d in (1, 3, 2):
        hid_in[d, 2, 0].wait_recv()
        hid_in[d, 2, 1].wait_recv()
        for copy in y_in[d]:
            copy.wait_recv()
        scale_block(turn(a, -d))

    p_in, c_in = {}, {}

    def send_parts(chunk, first, past):
        for copy in local[11 + first : 11 + past]:
            copy.wait()
        for d in (1, 3, 2):
            for copy in w_in[d][first:past]:
                copy.wait_recv()
        weights = wbuf[chunk]
        for d in (2, 1, 3, 0):
            to = turn(b, d)
            psend[chunk, d] = dot(scaled[quarter(to), :], weights).astype(BF16)
            if d:
                p_in[chunk, d] = sems.go(
                    psend.at[chunk, d], precv.at[chunk, d - 1], (kv_at(a, to), tp)
                )

    def send_sums(chunk):
        for d in (1, 3, 2):
            p_in[chunk, d].wait_recv()
        for d in (2, 1, 3, 0):
            to = turn(a, d)
            rows = pl.ds(pl.multiple_of(to * OWN, OWN), OWN)
            total = psend[chunk, 0, rows, :].astype(F32)
            for i in range(3):
                total = total + precv[chunk, i, rows, :].astype(F32)
            if d:
                csend[chunk, d - 1] = total.astype(BF16)
                c_in[chunk, d] = sems.go(csend.at[chunk, d - 1], proj.at[chunk, a], (kv_at(to, b), tp))
            else:
                proj[chunk, a] = total.astype(BF16)

    send_parts(0, 0, 4)
    s_in = {}
    ones = jnp.ones((8, KB), BF16)
    for d in (2, 1, 3, 0):
        to = turn(b, d)
        token = pl.ds(pl.multiple_of(kv_at(a, to) * OWN, OWN), OWN)
        mine = pl.ds(pl.multiple_of(to * 256 + a * OWN, OWN), OWN)
        write, decay = jnp.zeros((4, OWN), F32), jnp.zeros((4, OWN), F32)
        square = jnp.zeros((8, OWN), F32)
        for i in range(4):
            rows_i = scaled[mine, i * KB : (i + 1) * KB]
            write = write + lax.dot_general(wsm[i, 0], rows_i, NT, preferred_element_type=F32)
            decay = decay + lax.dot_general(wsm[i, 1], rows_i, NT, preferred_element_type=F32)
            h32 = hid[i, token, :].astype(F32)
            sq = h32 * h32
            high = sq.astype(BF16)
            low = (sq - high.astype(F32)).astype(BF16)
            square = square + lax.dot_general(ones, high, NT, preferred_element_type=F32)
            square = square + lax.dot_general(ones, low, NT, preferred_element_type=F32)
        part = jnp.concatenate([write, decay, square], 0)
        ssend[d] = jnp.concatenate([part, jnp.zeros((16, 64), F32)], 1)
        if d:
            s_in[d] = sems.go(ssend.at[d], srecv.at[d - 1], (kv_at(a, to), tp))
    send_parts(1, 4, 5)
    send_sums(0)
    send_parts(2, 5, 6)

    for d in (1, 3, 2):
        s_in[d].wait_recv()
    small = ssend[0]
    for i in range(3):
        small = small + srecv[i]
    small_cols = columns_of(small)
    inv_col = lax.rsqrt(small_cols[:, 8:9] / D + norm_eps)
    cols = rates_and_decays(small_cols[:, 0:8] * inv_col)
    send_sums(1)

    def new_keys(d):
        h = turn(a, -d)
        if d:
            c_in[0, d].wait_recv()
        bcol = pick(cols, h)
        c = running_sum(pick(cols, h + 4), at)
        w = decays(c, at)
        grow = jnp.exp(c)
        q = unit(silu(proj[0, h, :, 0:DK].astype(F32) * inv_col)) * DK ** (-0.5)
        k = unit(silu(proj[0, h, :, DK : 2 * DK].astype(F32) * inv_col))
        kl, ql = bcol * k * grow, q * grow
        for i in range(SEQ // 2):
            rows = slice(8 * i, 8 * i + 8)
            left = jnp.concatenate([kl[rows], ql[rows]], 0).astype(BF16)
            z0 = dot(left, st16[2 * i, h])
            z1 = dot(left, st16[2 * i + 1, h])
            zk[d, rows, :] = jnp.where(row8 < 4, z0[0:8], z1[0:8])
            zq[d, rows, :] = jnp.where(row8 < 4, z0[8:16], z1[8:16])
        t1, t2, t3 = inverse_rows(k, bcol, w)
        coef[d, 0], coef[d, 1], coef[d, 2] = t1, t2, t3
        for j in range(4):
            coef[d, 3 + j] = wide(jnp.sum(q * back(k, j), -1, keepdims=True), 128) * w[j]
        coef[d, 7] = bcol

    new_keys(0)
    new_keys(1)
    send_sums(2)
    new_keys(3)
    new_keys(2)

    def gated(ea, fb, d):
        src = turn(a, -ea)
        return gath.at[kv_at(src, turn(b, -fb)), turn(src, -d)]

    def along_a(s):
        return (kv_at(turn(a, s), b), tp)

    def along_b(s):
        return (kv_at(a, turn(b, s)), tp)

    def half_of(block, s):
        return block.at[pl.ds(OWN // 2 * (s // 2), OWN // 2), :]

    b_near, b_far = {}, {}
    first_in, peer_in, on_in = {}, {}, {}

    def new_rows(d):
        h = turn(a, -d)
        if d:
            c_in[1, d].wait_recv()
            c_in[2, d].wait_recv()
        v = silu(proj[1, h].astype(F32) * inv_col)
        fresh = mixed(both(coef[d, 7]) * v - zk[d], [both(coef[d, j]) for j in range(3)])
        res = zq[d]
        for j in range(4):
            res = res + both(coef[d, 3 + j]) * back(fresh, j)
        norm = res * lax.rsqrt(jnp.mean(res * res, -1, keepdims=True) + norm_eps) * head_gain_row[...]
        gath[kv, h] = (norm * silu(proj[2, h].astype(F32) * inv_col)).astype(BF16)

    def b_first(ea, d):
        block = gated(ea, 0, d)
        for s in (1, 3):
            b_near[ea, s, d] = sems.go(block, block, along_b(s))

    def b_relay(ea, d):
        for s in (1, 3):
            b_near[ea, s, d].wait_recv()
            block = half_of(gated(ea, s, d), s)
            b_far[ea, s, d] = sems.go(block, block, along_b(s))

    def start(d, direct=False):
        new_rows(d)
        block = gated(0, 0, d)
        for e in (2, 1, 3):
            first_in[e, d] = sems.go(block, block, along_a(e))
        if direct:
            for e in (2, 1, 3):
                peer_in[e, d] = sems.go(block, block, along_b(e))
        else:
            b_first(0, d)

    def hand_on(d, direct=False):
        for e in (1, 3, 2):
            first_in[e, d].wait_recv()
            if direct:
                block = gated(e, 0, d)
                for f in (2, 1, 3):
                    on_in[e, f, d] = sems.go(block, block, along_b(f))
            else:
                b_first(e, d)

    start(0)
    start(1)
    start(3, True)
    start(2, True)
    for d in (0, 1):
        b_relay(0, d)
        hand_on(d)
    hand_on(3, True)
    hand_on(2, True)
    for d in (0, 1):
        for e in (1, 3, 2):
            b_relay(e, d)

    def arrived(ea, fb):
        waits = []
        if fb == 2:
            waits += [b_far[ea, s, d] for d in (0, 1) for s in (1, 3)]
        if fb and ea:
            waits += [on_in[ea, fb, 3], on_in[ea, fb, 2]]
        elif fb:
            waits += [peer_in[fb, 3], peer_in[fb, 2]]
        return waits

    local[10].wait()
    weights = wo[...]
    outs = []

    def send_out(src, waits):
        n = len(outs)
        for copy in waits:
            copy.wait_recv()
        to, half = src // 2, lax.rem(src, 2)
        e = lax.rem(to - tp + 8, 8)
        rows = pl.ds(pl.multiple_of(half * OWN, OWN), OWN)
        total = dot(jnp.concatenate([gath[src, h] for h in range(HD)], 1), weights).astype(BF16)
        osend[n] = total
        copy = pltpu.make_async_remote_copy(
            src_ref=osend.at[n],
            dst_ref=orecv.at[e, rows, :],
            send_sem=o_send.at[n],
            recv_sem=o_recv.at[2 * e + half],
            device_id=(kv, to),
            device_id_type=MESH,
        )
        outs.append((e, copy))

        @pl.when(e != 0)
        def _():
            copy.start()

        @pl.when(e == 0)
        def _():
            orecv[0, rows, :] = total

    for ea, fb in ((0, 0), (1, 0), (3, 0), (2, 0), (0, 1), (0, 3), (0, 2)):
        send_out(kv_at(turn(a, -ea), turn(b, -fb)), arrived(ea, fb))
    for fb in (1, 3, 2):
        for ea in (1, 3, 2):
            send_out(kv_at(turn(a, -ea), turn(b, -fb)), arrived(ea, fb))

    for e in range(1, 8):
        for half in (0, 1):
            rows = pl.ds(half * OWN, OWN)
            pltpu.make_async_remote_copy(
                src_ref=osend.at[0],
                dst_ref=orecv.at[e, rows, :],
                send_sem=o_send.at[0],
                recv_sem=o_recv.at[2 * e + half],
                device_id=(kv, lax.rem(tp + e, 8)),
                device_id_type=MESH,
            ).wait_recv()
    for copy in sems.sent:
        copy.wait_send()
    for e, copy in outs:

        @pl.when(e != 0)
        def _():
            copy.wait_send()

    assert sems.at == N_SEM, sems.at


def mix(*args):
    hbm = pl.BlockSpec(memory_space=pl.ANY)
    vmem = pl.BlockSpec(memory_space=pltpu.VMEM)
    return pl.pallas_call(
        kernel,
        in_specs=[hbm] * 17,
        out_specs=(vmem, vmem),
        out_shape=(pltpu.VMEM((8, 128, 256), BF16), pltpu.VMEM((SEQ, HD, DK, DV), F32)),
        scratch_shapes=[
            pltpu.VMEM((32, 128), BF16),
            pltpu.VMEM((32, 128), F32),
            pltpu.VMEM((1, HD), F32),
            pltpu.VMEM((1, DV), F32),
            pltpu.VMEM((SEQ, 4, HD * DK), BF16),
            pltpu.VMEM((SEQ, 4, HD * DV), BF16),
            pltpu.VMEM((4, HD, SEQ), F32),
            pltpu.VMEM((4, HD, SEQ), F32),
            pltpu.VMEM((1, SEQ), jnp.int32),
            pltpu.VMEM((4, TOK, KB), BF16),
            pltpu.VMEM((TOK, 4 * KB), BF16),
            pltpu.VMEM((3, 4 * KB, 256), BF16),
            pltpu.VMEM((4, 2, 4, KB), BF16),
            pltpu.VMEM((SEQ, HD, DK, DV), BF16),
            pltpu.VMEM((HD * DV, 256), BF16),
            pltpu.VMEM((HD, OWN, 128), F32),
            pltpu.VMEM((HD, OWN, 128), F32),
            pltpu.VMEM((HD, OWN, DV), F32),
            pltpu.VMEM((HD, 3, OWN, 128), F32),
            pltpu.VMEM((HD, OWN, 128), F32),
            pltpu.VMEM((3, 4, 256, 256), BF16),
            pltpu.VMEM((3, 3, 256, 256), BF16),
            pltpu.VMEM((4, 16, 128), F32),
            pltpu.VMEM((3, 16, 128), F32),
            pltpu.VMEM((3, 3, OWN, 256), BF16),
            pltpu.VMEM((3, HD, OWN, 256), BF16),
            pltpu.VMEM((4, 8, OWN, 128), F32),
            pltpu.VMEM((4, OWN, DV), F32),
            pltpu.VMEM((4, OWN, DV), F32),
            pltpu.VMEM((16, HD, OWN, DV), BF16),
            pltpu.VMEM((16, OWN, 256), BF16),
            pltpu.SemaphoreType.DMA((N_SEM,)),
            pltpu.SemaphoreType.DMA((N_SEM,)),
            pltpu.SemaphoreType.DMA((17,)),
            pltpu.SemaphoreType.DMA((16,)),
            pltpu.SemaphoreType.DMA((16,)),
        ],
        compiler_params=pltpu.CompilerParams(
            collective_id=0, has_side_effects=True, vmem_limit_bytes=50 * 1024 * 1024
        ),
        name="mix",
    )(*[pltpu.with_memory_space_constraint(arg, pltpu.HBM) for arg in args])


def write_kernel(parts, states, out_ref, committed, rows, sem):
    copies = [pltpu.make_async_copy(states.at[n], committed.at[n], sem.at[n]) for n in range(SEQ)]
    for copy in copies:
        copy.start()
    total = parts[0].astype(F32)
    for i in range(1, 8):
        total = total + parts[i].astype(F32)
    rows[...] = total.astype(BF16)
    copy = pltpu.make_async_copy(rows, out_ref, sem.at[SEQ])
    copy.start()
    for other in copies:
        other.wait()
    copy.wait()


def write_out(parts, states):
    hbm = pl.BlockSpec(memory_space=pltpu.HBM)
    vmem = pl.BlockSpec(memory_space=pltpu.VMEM)
    return pl.pallas_call(
        write_kernel,
        in_specs=[vmem, vmem],
        out_specs=(hbm, hbm),
        out_shape=(jax.ShapeDtypeStruct((128, 256), BF16), jax.ShapeDtypeStruct((SEQ, HD, DK, DV), F32)),
        scratch_shapes=[pltpu.VMEM((128, 256), BF16), pltpu.SemaphoreType.DMA((SEQ + 1,))],
        compiler_params=pltpu.CompilerParams(vmem_limit_bytes=4 * 1024 * 1024),
        name="write_out",
    )(*[pltpu.with_memory_space_constraint(arg, pltpu.VMEM) for arg in (parts, states)])


def per_device(
    hidden,
    norm_gain,
    w_query,
    w_key,
    w_value,
    w_gate,
    w_write,
    w_decay,
    w_out,
    decay_rate,
    head_gain,
    carried_state,
    last_keys,
    last_values,
    last_writes,
    last_decays,
    accepted,
):
    parts, states = mix(
        hidden,
        norm_gain.reshape(32, 128),
        w_query,
        w_key,
        w_value,
        w_gate,
        w_write.T,
        w_decay.T,
        w_out,
        decay_rate.reshape(1, HD),
        head_gain.reshape(1, DV),
        carried_state,
        last_keys,
        last_values,
        jnp.transpose(last_writes, (1, 2, 0)),
        jnp.transpose(last_decays, (1, 2, 0)),
        accepted.reshape(1, SEQ),
    )
    return write_out(parts, states)


def solution(mesh):
    return jax.shard_map(
        per_device,
        mesh=mesh,
        in_specs=(
            P(None, "kv"),
            P(),
            P("kv", "tp"),
            P("kv", "tp"),
            P("kv", "tp"),
            P("kv", "tp"),
            P("kv", "tp"),
            P("kv", "tp"),
            P("tp", "kv"),
            P("tp"),
            P(),
            P("kv", "tp", None, None),
            P("kv", None, "tp"),
            P("kv", None, "tp"),
            P("kv", None, "tp"),
            P("kv", None, "tp"),
            P("kv"),
        ),
        out_specs=(P("tp", "kv"), P("kv", "tp", None, None)),
        check_vma=False,
    )
```
